32 devices in a mesh: ep: 4 (over y, x), tp: 8 (over z, core).
Axes of the slice: x: 2, y: 2, z: 4, core: 2. Of those that a mesh axis runs over, the one named last changes fastest.
Arguments:
- residual: bfloat16 [128, 2048], P('ep'), may hold values from -20 to 20
- cache_latent: bfloat16 [128, 2048, 256], P(('ep', 'tp')), may hold values from -12 to 12
- cache_rope: bfloat16 [128, 32, 2048], P(('ep', 'tp')), may hold values from -6 to 6
- lengths: int32 [128], P(('ep', 'tp')), may hold values from 2 to 2048, as said below
- query_latent: bfloat16 [128, 32, 256], P(('ep', 'tp')), may hold values from -250 to 250
- query_rope: bfloat16 [128, 32, 32], P(('ep', 'tp')), may hold values from -6 to 6
- norm_gain: bfloat16 [2048], replicated, may hold values from 0.099609375 to 1.8984375
- latent_weight: bfloat16 [2048, 256], replicated, may hold values from -0.125 to 0.125
- latent_gain: bfloat16 [256], replicated, may hold values from 0.099609375 to 1.8984375
- rope_weight: bfloat16 [32, 2048], replicated, may hold values from -0.125 to 0.125
- value_weight: bfloat16 [256, 2048], replicated, may hold values from -0.375 to 0.375
- out_weight: bfloat16 [2048, 2048], P('tp'), may hold values from -1 to 1
- mixer_gain: bfloat16 [2048], replicated, may hold values from 0.099609375 to 1.8984375
- group_router: bfloat16 [2048, 4], replicated, may hold values from -0.0625 to 0.0625
- expert_router: bfloat16 [2048, 8], replicated, may hold values from -0.0625 to 0.0625
- expert_ids: int32 [128, 2], P('ep'), may hold values from 0 to 7, as said below
- gate_weight: bfloat16 [8, 2048, 4096], P('ep', None, 'tp'), may hold values from -0.125 to 0.125
- up_weight: bfloat16 [8, 2048, 4096], P('ep', None, 'tp'), may hold values from -0.125 to 0.125
- down_weight: bfloat16 [8, 4096, 2048], P('ep', 'tp'), may hold values from -0.75 to 0.75
Outputs:
- mixed: bfloat16 [128, 2048], P('ep')
- new_latent: bfloat16 [128, 256], P(('ep', 'tp'))
- new_rope_key: bfloat16 [128, 32], P(('ep', 'tp'))
The draws below stay inside these ranges and needn't reach their ends.
Inputs may be any that keep to these rules, and one draw needn't show every extreme that they name: `lengths`: every sequence has 2 or more cached positions, and in every draw some sequence has all 2048. `expert_ids`: each row names 2 different experts of one group; group g holds experts g * 2 to g * 2 + 1. Among the rows of one index of ep (aligned blocks of 32 rows) no expert is named more than 16 times, and in every draw some expert is named exactly 16 times in every block.
All inputs are finite; a program needn't handle non-finite values.
Results may differ from the reference program's by a relative error of at most 0.012.
Values may be sent and summed in bfloat16 or wider, within the bound.
A program may use at most 64 MiB of HBM per device.

```python
import math
from functools import partial
import jax
import jax.numpy as jnp
from jax import lax

D = 2048
H = 32
KV = 256
ROPE = 32
NOPE = 64
V = 64
DE = 4096
GROUPS = 4
TOPK = 2
LEN = 2048
GROUP_SEQS = 32
SEQS = 128
EXPERTS = 8
CAP = 16
N_EP = 4


def anchor_rows(key):
    base_key = jax.random.fold_in(key, 7)
    first_rows = jax.random.normal(jax.random.fold_in(base_key, 1), (SEQS, KV), jnp.float32)
    other_rows = jax.random.normal(jax.random.fold_in(base_key, 2), (SEQS, KV), jnp.float32)
    return (first_rows, other_rows)


def draw_cache_latent(key, part):
    first_rows, other_rows = anchor_rows(key)
    remaining = jax.random.normal(jax.random.fold_in(key, 3), (SEQS, LEN - 2, KV), jnp.float32)
    whole = jnp.concatenate([first_rows[:, None, :], other_rows[:, None, :], remaining], axis=1)
    return jnp.clip(whole, -12.0, 12.0).astype(jnp.bfloat16)


def draw_query_latent(key, part):
    values = jax.random.normal(jax.random.fold_in(key, 5), (SEQS, H, KV), jnp.float32)
    return jnp.clip(values, -250.0, 250.0).astype(jnp.bfloat16)


def draw_residual(key, part):
    base_key = jax.random.fold_in(key, 13)
    column_scale = jnp.exp(jax.random.uniform(jax.random.fold_in(base_key, 1), (D,), jnp.float32, math.log(0.3), math.log(3.0)))
    values = jax.random.normal(jax.random.fold_in(base_key, 2), (SEQS, D), jnp.float32)
    return jnp.clip(values * column_scale[None, :], -20.0, 20.0).astype(jnp.bfloat16)


def draw_lengths(key, part):
    base_key = jax.random.fold_in(key, 17)
    exponent = jax.random.randint(jax.random.fold_in(base_key, 1), (SEQS,), 1, 14)
    spans = jnp.left_shift(jnp.ones((SEQS,), jnp.int32), exponent.astype(jnp.int32))
    drawn = 2 + jax.random.randint(jax.random.fold_in(base_key, 2), (SEQS,), 0, spans)
    drawn = jnp.minimum(drawn, LEN)
    chosen = jax.random.randint(jax.random.fold_in(base_key, 3), (), 0, SEQS)
    return jnp.where(jnp.arange(SEQS) == chosen, LEN, drawn).astype(jnp.int32)


def draw_expert_ids(key, part):
    base_key = jax.random.fold_in(key, 19)
    per_group = EXPERTS // GROUPS
    half_rows = GROUP_SEQS // 2
    busiest = jax.random.randint(jax.random.fold_in(base_key, 1), (), 0, GROUPS).astype(jnp.int32)

    def one_block(block_key):
        others = (busiest + jax.random.randint(jax.random.fold_in(block_key, 1), (GROUP_SEQS - half_rows,), 1, GROUPS)) % GROUPS
        chosen = jnp.concatenate([jnp.full((half_rows,), busiest, jnp.int32), others.astype(jnp.int32)])
        hit_table = (chosen[:, None] == jnp.arange(GROUPS, dtype=jnp.int32)[None, :]).astype(jnp.int32)
        order_in_group = jnp.sum((jnp.cumsum(hit_table, axis=0) - hit_table) * hit_table, axis=1)
        offsets = jax.random.randint(jax.random.fold_in(block_key, 2), (GROUPS,), 0, per_group)
        orders = jax.vmap(lambda sub_key: jax.random.permutation(sub_key, per_group))(jax.random.split(jax.random.fold_in(block_key, 3), GROUPS))
        first_slot = (offsets[chosen] + 2 * order_in_group) % per_group
        second_slot = (first_slot + 1) % per_group
        first_id = chosen * per_group + orders[chosen, first_slot]
        second_id = chosen * per_group + orders[chosen, second_slot]
        paired = jnp.stack([first_id, second_id], axis=1)
        shuffle = jax.random.permutation(jax.random.fold_in(block_key, 4), GROUP_SEQS)
        return paired[shuffle]
    block_keys = jax.random.split(jax.random.fold_in(base_key, 2), SEQS // GROUP_SEQS)
    return jax.vmap(one_block)(block_keys).reshape(SEQS, TOPK).astype(jnp.int32)


def spiked(values, stream_key, source, target, blocks, factor):
    owner, partner = [(jnp.arange(values.shape[dim]) // (values.shape[dim] // blocks)).reshape([-1 if axis == dim else 1 for axis in range(values.ndim)]) for dim in (source, target)]
    chosen = jax.random.permutation(stream_key, blocks)[partner]
    strong = (owner == chosen) | (owner == (partner + blocks // 2) % blocks)
    return jnp.where(strong, factor * values, values)


def block_scale(key, shape, pieces, low, largest):
    loudness, own = 1.0, jax.random.fold_in(key, 6)
    for dim, blocks in pieces:
        draws = jnp.exp(jax.random.uniform(jax.random.fold_in(own, dim), (blocks,), jnp.float32, low / len(pieces), largest / len(pieces)))
        loudness = loudness * jnp.repeat(draws, shape[dim] // blocks).reshape([-1 if axis == dim else 1 for axis in range(len(shape))])
    return loudness


def gaussian(key, extent, scale, reach, cuts=(), kind=jnp.bfloat16):
    values = jax.random.normal(key, extent, jnp.float32) * scale
    if len(cuts) > 0:
        values = block_scale(key, extent, cuts, -0.22, 0.18) * values
    return jnp.clip(values, min=-reach, max=reach).astype(kind)


def bell_draw_with(stream_key, dims, spread, limit, cuts, heavy, held_as=jnp.bfloat16):
    result = spread * jax.random.normal(stream_key, dims, jnp.float32)
    if cuts:
        result = result * block_scale(stream_key, dims, cuts, -0.22, 0.18)
    return jnp.clip(spiked(result, jax.random.fold_in(stream_key, 3), *heavy), -limit, limit).astype(held_as)


def setup_inputs(seed: int = 0) -> dict:
    splits = jax.random.split(jax.random.key(seed), 20)
    residual = draw_residual(jax.random.fold_in(splits[19], 71), 0)
    cache_latent = draw_cache_latent(jax.random.fold_in(splits[19], 71), 0)
    cache_rope = gaussian(splits[2], (SEQS, ROPE, LEN), 1.0, 6.0, ((0, 32),))
    lengths = draw_lengths(jax.random.fold_in(splits[19], 71), 0)
    query_latent = draw_query_latent(jax.random.fold_in(splits[19], 71), 0)
    query_rope = gaussian(splits[5], (SEQS, H, ROPE), 1.0, 6.0, ((0, 32),))
    norm_gain = jnp.clip(1.0 + 0.18 * jax.random.normal(splits[6], (D,), jnp.float32), 0.099609375, 1.8984375).astype(jnp.bfloat16)
    latent_weight = gaussian(splits[7], (D, KV), D ** -0.5, 0.125)
    latent_gain = jnp.clip(1.0 + 0.18 * jax.random.normal(splits[8], (KV,), jnp.float32), 0.099609375, 1.8984375).astype(jnp.bfloat16)
    rope_weight = gaussian(splits[9], (ROPE, D), D ** -0.5, 0.125)
    value_weight = gaussian(splits[10], (KV, H * V), KV ** -0.5, 0.375)
    out_weight = bell_draw_with(splits[11], (H * V, D), (H * V // 32) ** -0.5, 1.0, ((0, 8),), (0, 1, 8, 2.0))
    mixer_gain = jnp.clip(1.0 + 0.18 * jax.random.normal(splits[12], (D,), jnp.float32), 0.099609375, 1.8984375).astype(jnp.bfloat16)
    group_router = gaussian(splits[13], (D, GROUPS), (4 * D) ** -0.5, 0.0625)
    expert_router = gaussian(splits[14], (D, EXPERTS), (4 * D) ** -0.5, 0.0625)
    expert_ids = draw_expert_ids(jax.random.fold_in(splits[19], 71), 0)
    gate_weight = gaussian(splits[16], (EXPERTS, D, DE), D ** -0.5, 0.125, ((0, 4), (2, 8)))
    up_weight = gaussian(splits[17], (EXPERTS, D, DE), D ** -0.5, 0.125, ((0, 4), (2, 8)))
    down_weight = gaussian(splits[18], (EXPERTS, DE, D), (DE // 64) ** -0.5, 0.75, ((0, 4), (1, 8)))
    return {"residual": residual, "cache_latent": cache_latent, "cache_rope": cache_rope, "lengths": lengths, "query_latent": query_latent, "query_rope": query_rope, "norm_gain": norm_gain, "latent_weight": latent_weight, "latent_gain": latent_gain, "rope_weight": rope_weight, "value_weight": value_weight, "out_weight": out_weight, "mixer_gain": mixer_gain, "group_router": group_router, "expert_router": expert_router, "expert_ids": expert_ids, "gate_weight": gate_weight, "up_weight": up_weight, "down_weight": down_weight}


NORM_EPSILON = 1e-06
ROPE_BASE = 10000.0

def inverse_rms(values):
    return lax.rsqrt(lax.optimization_barrier(jnp.mean(values * values, axis=-1, keepdims=True)) + NORM_EPSILON)

def rotate(vector, position):
    half_width = vector.shape[-1] // 2
    frequency = ROPE_BASE ** (-jnp.arange(0, vector.shape[-1], 2, dtype=jnp.float32) / vector.shape[-1])
    angles = position[..., None] * frequency
    lower_half = vector[..., :half_width]
    upper_half = vector[..., half_width:]
    return jnp.concatenate([lower_half * jnp.cos(angles) - upper_half * jnp.sin(angles), upper_half * jnp.cos(angles) + lower_half * jnp.sin(angles)], axis=-1)

def dispatch_table(expert_rows, experts, capacity):
    flat_ids = expert_rows.reshape(-1)
    hit_table = (flat_ids[:, None] == jnp.arange(experts, dtype=jnp.int32)[None, :]).astype(jnp.int32)
    slot_rank = lax.optimization_barrier(jnp.sum((jnp.cumsum(hit_table, axis=0) - hit_table) * hit_table, axis=1))
    slot_index = flat_ids * capacity + slot_rank
    picked = (slot_index[None, :] == jnp.arange(experts * capacity, dtype=jnp.int32)[:, None]).astype(jnp.float32)
    return picked.reshape(experts * capacity, expert_rows.shape[0], expert_rows.shape[1])

def route_weights(expert_in, group_router, expert_router, expert_ids, per_group):
    group_logits = jnp.dot(expert_in, group_router, preferred_element_type=jnp.float32)
    expert_logits = jnp.dot(expert_in, expert_router, preferred_element_type=jnp.float32)
    chosen = expert_ids[:, 0] // per_group
    group_hit = (jnp.arange(group_logits.shape[1], dtype=jnp.int32)[None, :] == chosen[:, None]).astype(jnp.float32)
    chosen_logit = lax.optimization_barrier(jnp.sum(group_logits * group_hit, axis=1, keepdims=True))
    group_share = 1.0 / lax.optimization_barrier(jnp.sum(jnp.exp(group_logits - chosen_logit), axis=1))
    expert_hit = (expert_ids[:, :, None] == jnp.arange(expert_logits.shape[1], dtype=jnp.int32)[None, None, :]).astype(jnp.float32)
    picked_logit = lax.optimization_barrier(jnp.sum(expert_hit * expert_logits[:, None, :], axis=2))
    inner_share = 1.0 / lax.optimization_barrier(jnp.sum(jnp.exp(picked_logit[:, None, :] - picked_logit[:, :, None]), axis=2))
    return group_share[:, None] * inner_share

def attend_one(args):
    latent_rows, rope_rows, length, query_lat, query_rot, fresh_latent, fresh_rope = args
    score_scale = (NOPE + ROPE) ** (-0.5)
    cached = (jnp.dot(query_lat, latent_rows.T, preferred_element_type=jnp.float32) + jnp.dot(query_rot, rope_rows, preferred_element_type=jnp.float32)) * score_scale
    keeping = jnp.arange(latent_rows.shape[0], dtype=jnp.int32) < length
    cached = jnp.where(keeping[None, :], cached, -jnp.inf)
    fresh = (jnp.dot(query_lat, fresh_latent, preferred_element_type=jnp.float32) + jnp.dot(query_rot, fresh_rope, preferred_element_type=jnp.float32)) * score_scale
    row_top = jnp.maximum(lax.optimization_barrier(jnp.max(cached, axis=1)), fresh)
    cached_exp = jnp.exp(cached - row_top[:, None])
    fresh_exp = jnp.exp(fresh - row_top)
    denominator = lax.optimization_barrier(jnp.sum(cached_exp, axis=1)) + fresh_exp
    cached_weight = (cached_exp / denominator[:, None]).astype(jnp.bfloat16)
    fresh_weight = (fresh_exp / denominator).astype(jnp.bfloat16)
    combined = jnp.dot(cached_weight, latent_rows, preferred_element_type=jnp.float32) + fresh_weight.astype(jnp.float32)[:, None] * fresh_latent.astype(jnp.float32)[None, :]
    return combined.astype(jnp.bfloat16)

def run_expert(args):
    rows, gate_part, up_part, down_part = args
    gate_value = jnp.dot(rows, gate_part, preferred_element_type=jnp.float32)
    up_value = jnp.dot(rows, up_part, preferred_element_type=jnp.float32)
    activation = (jax.nn.silu(gate_value) * up_value).astype(jnp.bfloat16)
    return jnp.dot(activation, down_part, preferred_element_type=jnp.float32)

def reference(residual, cache_latent, cache_rope, lengths, query_latent, query_rope, norm_gain, latent_weight, latent_gain, rope_weight, value_weight, out_weight, mixer_gain, group_router, expert_router, expert_ids, gate_weight, up_weight, down_weight):
    resid_f = residual.astype(jnp.float32)
    normed = (resid_f * inverse_rms(resid_f) * norm_gain.astype(jnp.float32)).astype(jnp.bfloat16)
    latent_raw = jnp.dot(normed, latent_weight, preferred_element_type=jnp.float32)
    new_latent = (latent_raw * inverse_rms(latent_raw) * latent_gain.astype(jnp.float32)).astype(jnp.bfloat16)
    positions = lengths.astype(jnp.float32)
    rope_raw = jnp.dot(normed, rope_weight.T, preferred_element_type=jnp.float32)
    new_rope_key = rotate(rope_raw, positions).astype(jnp.bfloat16)
    query_turned = rotate(query_rope.astype(jnp.float32), positions[:, None]).astype(jnp.bfloat16)
    mixed_latent = lax.map(attend_one, (cache_latent, cache_rope, lengths, query_latent, query_turned, new_latent, new_rope_key))
    head_values = jnp.einsum('shc,chv->shv', mixed_latent.astype(jnp.float32), value_weight.reshape(KV, H, V).astype(jnp.float32)).astype(jnp.bfloat16)
    attended = jnp.dot(head_values.reshape(SEQS, H * V), out_weight, preferred_element_type=jnp.float32)
    after_attention = (resid_f + attended).astype(jnp.bfloat16)
    after_f = after_attention.astype(jnp.float32)
    expert_in = (after_f * inverse_rms(after_f) * mixer_gain.astype(jnp.float32)).astype(jnp.bfloat16)
    route_weight = route_weights(expert_in, group_router, expert_router, expert_ids, EXPERTS // GROUPS)
    ids_blocks = expert_ids.reshape(N_EP, GROUP_SEQS, TOPK)
    picked = jax.vmap(partial(dispatch_table, experts=EXPERTS, capacity=CAP))(ids_blocks)
    select_rows = lax.optimization_barrier(jnp.sum(picked, axis=3))
    outbound = jnp.einsum('bsr,brd->bsd', select_rows, expert_in.reshape(N_EP, GROUP_SEQS, D).astype(jnp.float32), precision=lax.Precision.HIGHEST).astype(jnp.bfloat16)
    per_expert = outbound.reshape(N_EP, EXPERTS, CAP, D).transpose(1, 0, 2, 3).reshape(EXPERTS, N_EP * CAP, D)
    expert_out = lax.map(run_expert, (per_expert, gate_weight, up_weight, down_weight))
    back_blocks = expert_out.reshape(EXPERTS, N_EP, CAP, D).transpose(1, 0, 2, 3).reshape(N_EP, EXPERTS * CAP, D)
    combine = lax.optimization_barrier(jnp.sum(picked * route_weight.reshape(N_EP, 1, GROUP_SEQS, TOPK), axis=3))
    moe_sum = jnp.einsum('bsr,bsd->brd', combine, back_blocks, precision=lax.Precision.HIGHEST).reshape(SEQS, D)
    mixed = (after_f + moe_sum).astype(jnp.bfloat16)
    return (mixed, new_latent, new_rope_key)
```

```python
import functools

import jax
import jax.numpy as jnp
from jax import lax
from jax.experimental import pallas as pl
from jax.experimental.pallas import tpu as pltpu
from jax.sharding import PartitionSpec as P

NORM_EPSILON = 1e-06
ROPE_BASE = 10000.0
TOPK = 2

F32 = jnp.float32
BF16 = jnp.bfloat16


def dot(a, b, contract=((1,), (0,)), precision=None):
    return lax.dot_general(
        a, b, (contract, ((), ())), preferred_element_type=F32, precision=precision
    )


def inverse_rms(values):
    return lax.rsqrt(jnp.mean(values * values, axis=-1, keepdims=True) + NORM_EPSILON)


def iota(shape, dim):
    return lax.broadcasted_iota(jnp.int32, shape, dim)


def layer(
    sizes,
    residual,
    cache_latent,
    cache_rope,
    lengths,
    query_latent,
    query_rope,
    norm_gain,
    latent_weight,
    latent_gain,
    rope_weight,
    value_weight,
    out_weight,
    mixer_gain,
    group_router,
    expert_router,
    expert_ids,
    gate_weight,
    up_weight,
    down_weight,
    mixed_out,
    latent_out,
    rope_out,
    residual_v,
    cache_v,
    rope_v,
    query_v,
    query_rope_v,
    norm_gain_v,
    latent_weight_v,
    latent_gain_v,
    rope_weight_v,
    value_v,
    out_v,
    mixer_gain_v,
    group_router_v,
    expert_router_v,
    ids_v,
    gate_v,
    up_v,
    down_v,
    head_send,
    head_recv,
    meta_send,
    meta_recv,
    sum_send,
    sum_recv,
    disp_send,
    disp_recv,
    ret_send,
    ret_recv,
    share_send,
    share_recv,
    load_sem,
    cache_sem,
    rope_sem,
    expert_sem,
    head_sems,
    meta_sems,
    sum_sems,
    disp_sems,
    ret_sems,
    share_sems,
):
    n_ep, n_tp, slots, scale = sizes
    n_dev = n_ep * n_tp
    rows, width = residual_v.shape
    seqs, heads, latent = query_v.shape
    rope_width = rope_weight_v.shape[0]
    half = rope_width // 2
    length = cache_v.shape[1]
    pad = head_send.shape[1]
    head_cols = head_send.shape[2]
    col = width // n_tp
    local_experts = gate_v.shape[0]
    experts = expert_router_v.shape[0]
    groups = group_router_v.shape[0]
    per_group = experts // groups
    value_dim = value_v.shape[1] // heads

    my_e = lax.axis_index("ep")
    my_t = lax.axis_index("tp")
    me = my_e * n_tp + my_t

    loads = [
        pltpu.make_async_copy(src, dst, load_sem.at[i])
        for i, (src, dst) in enumerate(
            [
                (residual, residual_v),
                (norm_gain, norm_gain_v),
                (latent_weight, latent_weight_v),
                (latent_gain, latent_gain_v),
                (rope_weight, rope_weight_v),
                (query_rope, query_rope_v),
                (query_latent, query_v),
                (expert_ids, ids_v),
                (value_weight, value_v),
                (out_weight, out_v),
                (mixer_gain, mixer_gain_v),
                (group_router, group_router_v),
                (expert_router, expert_router_v),
            ]
        )
    ]
    caches = [
        pltpu.make_async_copy(cache_latent.at[s], cache_v.at[s], cache_sem.at[s])
        for s in range(seqs)
    ]
    ropes = [
        pltpu.make_async_copy(cache_rope.at[s], rope_v.at[s], rope_sem.at[s])
        for s in range(seqs)
    ]
    expert_loads = [
        [
            pltpu.make_async_copy(src.at[l], dst.at[l], expert_sem.at[k, l])
            for l in range(local_experts)
        ]
        for k, (src, dst) in enumerate(
            [(gate_weight, gate_v), (up_weight, up_v), (down_weight, down_v)]
        )
    ]
    for load in loads[:8]:
        load.start()
    for s in range(seqs):
        ropes[s].start()
        caches[s].start()
    for load in loads[8:]:
        load.start()
    for kind in expert_loads:
        for load in kind:
            load.start()

    barrier = pltpu.get_barrier_semaphore()

    def device(t):
        return {"ep": t // n_tp, "tp": lax.rem(t, n_tp)}

    def greet(i, carry):
        pl.semaphore_signal(
            barrier,
            inc=1,
            device_id=device(lax.rem(me + i, n_dev)),
            device_id_type=pl.DeviceIdType.MESH,
        )
        return carry

    lax.fori_loop(1, n_dev, greet, 0)

    def remote(src, dst, send_sem, recv_sem, e, t):
        return pltpu.make_async_remote_copy(
            src_ref=src,
            dst_ref=dst,
            send_sem=send_sem,
            recv_sem=recv_sem,
            device_id={"ep": e, "tp": t},
            device_id_type=pl.DeviceIdType.MESH,
        )

    loads[7].wait()
    id0 = ids_v[0:1, :]
    id1 = ids_v[1:2, :]
    low = iota((n_ep, rows), 0) * local_experts
    high = low + local_experts
    hits = jnp.where(
        ((id0 >= low) & (id0 < high)) | ((id1 >= low) & (id1 < high)), 1.0, 0.0
    ).astype(F32)
    before = jnp.where(iota((rows, rows), 0) < iota((rows, rows), 1), 1.0, 0.0).astype(BF16)
    rank = dot(hits.astype(BF16), before)
    slot_of = jnp.where(hits > 0.5, rank, -1.0)
    slot_row = iota((slots, rows), 0).astype(F32)
    select = jnp.concatenate(
        [jnp.where(slot_row == slot_of[d : d + 1, :], 1.0, 0.0).astype(F32) for d in range(n_ep)],
        axis=0,
    )
    tag0 = jnp.sum(select * (id0.astype(F32) + 1.0), axis=1, keepdims=True)
    tag1 = jnp.sum(select * (id1.astype(F32) + 1.0), axis=1, keepdims=True)
    lane = iota((n_ep * slots, 128), 1)
    tags = jnp.where(lane == 0, tag0, jnp.where(lane == 1, tag1, 0.0))
    for d in range(n_ep):
        meta_send[d] = tags[d * slots : (d + 1) * slots]
    meta_recv[my_e] = meta_send[my_e]
    select_b = select.astype(BF16)

    for i in (0, 1, 2, 3, 4, 5, 6):
        loads[i].wait()
    resid = residual_v[...].astype(F32)
    gain = norm_gain_v[...].astype(F32).reshape(1, width)
    normed_all = (resid * inverse_rms(resid) * gain).astype(BF16)
    own = jnp.where(
        iota((seqs, rows), 1) == my_t * seqs + iota((seqs, rows), 0), 1.0, 0.0
    ).astype(BF16)
    normed = dot(own, normed_all).astype(BF16)
    latent_raw = dot(normed, latent_weight_v[...])
    new_latent = (
        latent_raw * inverse_rms(latent_raw) * latent_gain_v[...].astype(F32).reshape(1, latent)
    ).astype(BF16)
    position = jnp.zeros((seqs, 1), F32)
    for s in range(seqs):
        position = jnp.where(iota((seqs, 1), 0) == s, lengths[s].astype(F32), position)
    index = iota((1, rope_width), 1)
    index = jnp.where(index >= half, index - half, index).astype(F32)
    frequency = jnp.power(jnp.full((1, rope_width), ROPE_BASE, F32), -2.0 * index / rope_width)
    angles = position * frequency
    cosine = jnp.cos(angles)
    sine = jnp.sin(angles)
    weight_r = rope_weight_v[...]
    swapped = jnp.concatenate([-weight_r[half:], weight_r[:half]], axis=0)
    new_rope = (
        dot(normed, weight_r, ((1,), (1,))) * cosine + dot(normed, swapped, ((1,), (1,))) * sine
    ).astype(BF16)
    latent_out[...] = new_latent
    rope_out[...] = new_rope
    source = iota((rope_width, rope_width), 0)
    target = iota((rope_width, rope_width), 1)
    turn = (
        jnp.where(source + half == target, 1.0, 0.0) - jnp.where(source == target + half, 1.0, 0.0)
    ).astype(BF16)

    new_latent_f = new_latent.astype(F32)
    new_rope_f = new_rope.astype(F32)
    mixed_latents = []
    for s in range(seqs):
        query = query_v[s]
        query_r = query_rope_v[s]
        turned = (
            query_r.astype(F32) * cosine[s : s + 1] + dot(query_r, turn) * sine[s : s + 1]
        ).astype(BF16)
        fresh_latent = new_latent_f[s : s + 1]
        fresh = (
            jnp.sum(query.astype(F32) * fresh_latent, axis=1, keepdims=True)
            + jnp.sum(turned.astype(F32) * new_rope_f[s : s + 1], axis=1, keepdims=True)
        ) * scale
        ropes[s].wait()
        caches[s].wait()
        score = (dot(query, cache_v[s], ((1,), (1,))) + dot(turned, rope_v[s])) * scale
        score = jnp.where(iota((heads, length), 1) < lengths[s], score, -jnp.inf)
        top = jnp.maximum(jnp.max(score, axis=1, keepdims=True), fresh)
        powers = jnp.exp(score - top)
        fresh_power = jnp.exp(fresh - top)
        inverse = 1.0 / (jnp.sum(powers, axis=1, keepdims=True) + fresh_power)
        weight = (powers * inverse).astype(BF16)
        fresh_weight = (fresh_power * inverse).astype(BF16).astype(F32)
        mixed_latents.append(
            (dot(weight, cache_v[s]) + fresh_weight * fresh_latent).astype(BF16)
        )
    lhs = jnp.concatenate(mixed_latents, axis=0)

    loads[8].wait()
    for t in range(n_tp):
        found = dot(lhs, value_v[:, t * head_cols : (t + 1) * head_cols])
        head = iota((heads, head_cols), 0)
        column = iota((heads, head_cols), 1) + t * head_cols
        mine = (column >= head * value_dim) & (column < (head + 1) * value_dim)
        block = jnp.zeros((pad, head_cols), F32)
        for s in range(seqs):
            line = jnp.sum(
                jnp.where(mine, found[s * heads : (s + 1) * heads], 0.0), axis=0, keepdims=True
            )
            block = jnp.where(iota((pad, head_cols), 0) == s, line, block)
        head_send[t] = block
    pl.semaphore_wait(barrier, n_dev - 1)
    for i in range(1, n_tp):
        t = lax.rem(my_t + i, n_tp)
        remote(
            head_send.at[t], head_recv.at[my_t], head_sems.at[0, t], head_sems.at[1, my_t], my_e, t
        ).start()
    for i in range(1, n_ep):
        e = lax.rem(my_e + i, n_ep)
        remote(
            meta_send.at[e], meta_recv.at[my_e], meta_sems.at[0, e], meta_sems.at[1, my_e], e, my_t
        ).start()
    head_recv[my_t] = head_send[my_t]
    loads[9].wait()
    line = iota((rows, n_tp * pad), 0)
    spot = iota((rows, n_tp * pad), 1)
    inner = spot & (pad - 1)
    outer = lax.shift_right_logical(spot, pad.bit_length() - 1)
    gather = jnp.where((inner < seqs) & (line == outer * seqs + inner), 1.0, 0.0).astype(BF16)
    for i in range(1, n_tp):
        t = lax.rem(my_t + i, n_tp)
        remote(
            head_send.at[t], head_recv.at[t], head_sems.at[0, t], head_sems.at[1, t], my_e, t
        ).wait()
    by_heads = dot(
        gather, head_recv[...].reshape(n_tp * pad, head_cols).astype(BF16)
    ).astype(BF16)

    for i in range(1, n_tp + 1):
        t = lax.rem(my_t + i, n_tp)
        cols = pl.ds(pl.multiple_of(t * col, col), col)
        sum_send[t] = dot(by_heads, out_v[:, cols]).astype(BF16)
        if i < n_tp:
            remote(
                sum_send.at[t], sum_recv.at[my_t], sum_sems.at[0, t], sum_sems.at[1, my_t], my_e, t
            ).start()
    my_cols = pl.ds(pl.multiple_of(my_t * col, col), col)
    attended = sum_send[my_t].astype(F32)
    for i in range(1, n_tp):
        t = lax.rem(my_t + n_tp - i, n_tp)
        remote(
            sum_send.at[t], sum_recv.at[t], sum_sems.at[0, t], sum_sems.at[1, t], my_e, t
        ).wait()
        attended = attended + sum_recv[t].astype(F32)
    after = (residual_v[:, my_cols].astype(F32) + attended).astype(BF16)

    chosen = dot(select_b, after).astype(BF16)
    for d in range(n_ep):
        disp_send[d] = chosen[d * slots : (d + 1) * slots]
    disp_recv[my_e, my_t] = disp_send[my_e]

    def send_rows(i, carry):
        to = lax.rem(me + i, n_dev)
        e = to // n_tp
        t = lax.rem(to, n_tp)
        remote(
            disp_send.at[e],
            disp_recv.at[my_e, my_t],
            disp_sems.at[0, e, t],
            disp_sems.at[1, my_e, my_t],
            e,
            t,
        ).start()
        return carry

    lax.fori_loop(1, n_dev, send_rows, 0)
    for load in loads[10:13]:
        load.wait()

    def await_rows(i, carry):
        to = lax.rem(me + n_dev - i, n_dev)
        e = to // n_tp
        t = lax.rem(to, n_tp)
        remote(
            disp_send.at[e], disp_recv.at[e, t], disp_sems.at[0, e, t], disp_sems.at[1, e, t], e, t
        ).wait()
        return carry

    for i in range(1, n_ep):
        e = lax.rem(my_e + i, n_ep)
        remote(
            meta_send.at[e], meta_recv.at[e], meta_sems.at[0, e], meta_sems.at[1, e], e, my_t
        ).wait()
    lax.fori_loop(1, n_dev, await_rows, 0)
    total = n_ep * slots
    taken = jnp.concatenate(
        [disp_recv[:, t].reshape(total, col) for t in range(n_tp)], axis=1
    ).astype(F32)
    mixer = mixer_gain_v[...].astype(F32).reshape(1, width)
    expert_in = (taken * inverse_rms(taken) * mixer).astype(BF16)
    group_logits = dot(expert_in, group_router_v[...], ((1,), (1,)))
    expert_logits = dot(expert_in, expert_router_v[...], ((1,), (1,)))
    meta = meta_recv[...].reshape(total, 128)
    name0 = meta[:, 0:1] - 1.0
    name1 = meta[:, 1:2] - 1.0
    group_low = (iota((total, groups), 1) * per_group).astype(F32)
    in_group = (name0 >= group_low) & (name0 < group_low + per_group)
    group_top = jnp.sum(jnp.where(in_group, group_logits, 0.0), axis=1, keepdims=True)
    share = 1.0 / jnp.sum(jnp.exp(group_logits - group_top), axis=1, keepdims=True)
    number = iota((total, experts), 1).astype(F32)
    pick0 = jnp.sum(jnp.where(number == name0, expert_logits, 0.0), axis=1, keepdims=True)
    pick1 = jnp.sum(jnp.where(number == name1, expert_logits, 0.0), axis=1, keepdims=True)
    route0 = share / (1.0 + jnp.exp(pick1 - pick0))
    route1 = share / (1.0 + jnp.exp(pick0 - pick1))

    acts = []
    routes = []
    for l in range(local_experts):
        name = (my_e * local_experts + l).astype(F32)
        routes.append(
            jnp.where(name0 == name, route0, 0.0) + jnp.where(name1 == name, route1, 0.0)
        )
        expert_loads[0][l].wait()
        gate = dot(expert_in, gate_v[l])
        expert_loads[1][l].wait()
        up = dot(expert_in, up_v[l])
        acts.append((gate / (1.0 + jnp.exp(-gate)) * up).astype(BF16))
    for load in expert_loads[2]:
        load.wait()
    for i in range(1, n_tp + 1):
        t = lax.rem(my_t + i, n_tp)
        cols = pl.ds(pl.multiple_of(t * col, col), col)
        part = jnp.zeros((total, col), F32)
        for l in range(local_experts):
            part = part + routes[l] * dot(acts[l], down_v[l, :, cols])
        part = part.astype(BF16)
        for e in range(n_ep):
            ret_send[e, t] = part[e * slots : (e + 1) * slots]
        for k in range(1 if i == n_tp else 0, n_ep):
            e = lax.rem(my_e + k, n_ep)
            remote(
                ret_send.at[e, t],
                ret_recv.at[my_e, my_t],
                ret_sems.at[0, e, t],
                ret_sems.at[1, my_e, my_t],
                e,
                t,
            ).start()
    ret_recv[my_e, my_t] = ret_send[my_e, my_t]

    def await_sums(i, carry):
        to = lax.rem(me + n_dev - i, n_dev)
        e = to // n_tp
        t = lax.rem(to, n_tp)
        remote(
            ret_send.at[e, t], ret_recv.at[e, t], ret_sems.at[0, e, t], ret_sems.at[1, e, t], e, t
        ).wait()
        return carry

    lax.fori_loop(1, n_dev, await_sums, 0)
    gathered = ret_recv[:, 0].astype(F32)
    for t in range(1, n_tp):
        gathered = gathered + ret_recv[:, t].astype(F32)
    moe = dot(
        select, gathered.reshape(total, col), ((0,), (0,)), precision=lax.Precision.HIGHEST
    )
    share_send[...] = (after.astype(F32) + moe).astype(BF16)
    for i in range(1, n_tp):
        t = lax.rem(my_t + i, n_tp)
        remote(
            share_send, share_recv.at[my_t], share_sems.at[0, t], share_sems.at[1, my_t], my_e, t
        ).start()
    share_recv[my_t] = share_send[...]
    for i in range(1, n_tp):
        t = lax.rem(my_t + n_tp - i, n_tp)
        remote(
            share_send, share_recv.at[t], share_sems.at[0, t], share_sems.at[1, t], my_e, t
        ).wait()
    for t in range(n_tp):
        mixed_out[:, t * col : (t + 1) * col] = share_recv[t]


def on_device(n_ep, n_tp, *args):
    (
        residual,
        cache_latent,
        cache_rope,
        lengths,
        query_latent,
        query_rope,
        norm_gain,
        latent_weight,
        latent_gain,
        rope_weight,
        value_weight,
        out_weight,
        mixer_gain,
        group_router,
        expert_router,
        expert_ids,
        gate_weight,
        up_weight,
        down_weight,
    ) = args
    rows, width = residual.shape
    seqs, heads, latent = query_latent.shape
    rope_width = query_rope.shape[2]
    local_experts = gate_weight.shape[0]
    experts = expert_router.shape[1]
    per_group = experts // group_router.shape[1]
    capacity = 2 * rows * TOPK // experts
    slots = capacity if per_group == TOPK == local_experts else min(local_experts * capacity, rows)
    slots = -(-slots // 16) * 16
    col = width // n_tp
    head_cols = out_weight.shape[0]
    pad = 8
    while pad < seqs:
        pad *= 2
    value_dim = value_weight.shape[1] // heads
    scale = float((value_dim + rope_width) ** (-0.5))
    group_router = group_router.T
    expert_router = expert_router.T
    expert_ids = expert_ids.T
    hbm = pl.BlockSpec(memory_space=pl.ANY)
    vmem = pl.BlockSpec(memory_space=pltpu.VMEM)
    smem = pl.BlockSpec(memory_space=pltpu.SMEM)

    def held(array):
        return pltpu.VMEM(array.shape, array.dtype)

    dma = pltpu.SemaphoreType.DMA
    return pl.pallas_call(
        functools.partial(layer, (n_ep, n_tp, slots, scale)),
        out_shape=(
            jax.ShapeDtypeStruct((rows, width), BF16),
            jax.ShapeDtypeStruct((seqs, latent), BF16),
            jax.ShapeDtypeStruct((seqs, rope_width), BF16),
        ),
        in_specs=[hbm] * 3 + [smem] + [hbm] * 15,
        out_specs=(vmem, vmem, vmem),
        scratch_shapes=[
            held(residual),
            held(cache_latent),
            held(cache_rope),
            held(query_latent),
            held(query_rope),
            held(norm_gain),
            held(latent_weight),
            held(latent_gain),
            held(rope_weight),
            held(value_weight),
            held(out_weight),
            held(mixer_gain),
            held(group_router),
            held(expert_router),
            held(expert_ids),
            held(gate_weight),
            held(up_weight),
            held(down_weight),
            pltpu.VMEM((n_tp, pad, head_cols), F32),
            pltpu.VMEM((n_tp, pad, head_cols), F32),
            pltpu.VMEM((n_ep, slots, 128), F32),
            pltpu.VMEM((n_ep, slots, 128), F32),
            pltpu.VMEM((n_tp, rows, col), BF16),
            pltpu.VMEM((n_tp, rows, col), BF16),
            pltpu.VMEM((n_ep, slots, col), BF16),
            pltpu.VMEM((n_ep, n_tp, slots, col), BF16),
            pltpu.VMEM((n_ep, n_tp, slots, col), BF16),
            pltpu.VMEM((n_ep, n_tp, slots, col), BF16),
            pltpu.VMEM((rows, col), BF16),
            pltpu.VMEM((n_tp, rows, col), BF16),
            dma((13,)),
            dma((seqs,)),
            dma((seqs,)),
            dma((3, local_experts)),
            dma((2, n_tp)),
            dma((2, n_ep)),
            dma((2, n_tp)),
            dma((2, n_ep, n_tp)),
            dma((2, n_ep, n_tp)),
            dma((2, n_tp)),
        ],
        compiler_params=pltpu.CompilerParams(collective_id=0, has_side_effects=True),
        name="layer",
    )(
        residual,
        cache_latent,
        cache_rope,
        lengths,
        query_latent,
        query_rope,
        norm_gain,
        latent_weight,
        latent_gain,
        rope_weight,
        value_weight,
        out_weight,
        mixer_gain,
        group_router,
        expert_router,
        expert_ids,
        gate_weight,
        up_weight,
        down_weight,
    )


def solution(mesh):
    in_specs = (
        P("ep", None),
        P(("ep", "tp"), None, None),
        P(("ep", "tp"), None, None),
        P(("ep", "tp")),
        P(("ep", "tp"), None, None),
        P(("ep", "tp"), None, None),
        P(),
        P(),
        P(),
        P(),
        P(),
        P("tp", None),
        P(),
        P(),
        P(),
        P("ep", None),
        P("ep", None, "tp"),
        P("ep", None, "tp"),
        P("ep", "tp", None),
    )
    out_specs = (P("ep", None), P(("ep", "tp"), None), P(("ep", "tp"), None))
    return jax.shard_map(
        functools.partial(on_device, mesh.shape["ep"], mesh.shape["tp"]),
        mesh=mesh,
        in_specs=in_specs,
        out_specs=out_specs,
        check_vma=False,
    )
```

```python
import functools

import jax
import jax.numpy as jnp
from jax import lax
from jax.experimental import pallas as pl
from jax.experimental.pallas import tpu as pltpu
from jax.sharding import PartitionSpec as P

NORM_EPSILON = 1e-06
ROPE_BASE = 10000.0
TOPK = 2

F32 = jnp.float32
BF16 = jnp.bfloat16


def dot(a, b, contract=((1,), (0,)), precision=None):
    return lax.dot_general(
        a, b, (contract, ((), ())), preferred_element_type=F32, precision=precision
    )


def inverse_rms(values):
    return lax.rsqrt(jnp.mean(values * values, axis=-1, keepdims=True) + NORM_EPSILON)


def iota(shape, dim):
    return lax.broadcasted_iota(jnp.int32, shape, dim)


def layer(
    sizes,
    residual,
    cache_latent,
    cache_rope,
    lengths_hbm,
    query_latent,
    query_rope,
    norm_gain,
    latent_weight,
    latent_gain,
    rope_weight,
    value_weight,
    out_weight,
    mixer_gain,
    group_router,
    expert_router,
    expert_ids,
    gate_weight,
    up_weight,
    down_weight,
    mixed_out,
    latent_out,
    rope_out,
    lengths,
    residual_v,
    cache_v,
    rope_v,
    query_v,
    query_rope_v,
    norm_gain_v,
    latent_weight_v,
    latent_gain_v,
    rope_weight_v,
    value_v,
    out_v,
    mixer_gain_v,
    group_router_v,
    expert_router_v,
    ids_v,
    gate_v,
    up_v,
    down_v,
    head_send,
    head_recv,
    meta_send,
    meta_recv,
    half_send,
    half_recv,
    sum_send,
    sum_recv,
    disp_send,
    disp_recv,
    pair_send,
    pair_recv,
    ret_send,
    ret_recv,
    share_send,
    share_recv,
    latent_v,
    rope_key_v,
    length_sem,
    load_sem,
    cache_sem,
    rope_sem,
    expert_sem,
    head_sems,
    meta_sems,
    half_sems,
    sum_sems,
    disp_sems,
    pass_sems,
    pair_sems,
    ret_sems,
    share_sems,
    store_sem,
):
    n_ep, n_tp, slots, scale = sizes
    rows, width = residual_v.shape
    seqs, heads, latent = query_v.shape
    rope_width = rope_weight_v.shape[0]
    half = rope_width // 2
    length = cache_v.shape[1]
    pad = head_send.shape[1]
    head_cols = head_send.shape[2]
    col = width // n_tp
    local_experts = gate_v.shape[0]
    experts = expert_router_v.shape[0]
    groups = group_router_v.shape[0]
    per_group = experts // groups
    value_dim = value_v.shape[1] // heads

    my_e = lax.axis_index("ep")
    my_t = lax.axis_index("tp")
    n_z = n_tp // 2
    my_z = my_t // 2
    core = lax.rem(my_t, 2)
    sibling = my_t + 1 - 2 * core
    n_chip = n_ep * n_z
    my_chip = my_e * n_z + my_z

    loads = [
        pltpu.make_async_copy(src, dst, load_sem.at[i])
        for i, (src, dst) in enumerate(
            [
                (residual, residual_v),
                (norm_gain, norm_gain_v),
                (latent_weight, latent_weight_v),
                (latent_gain, latent_gain_v),
                (rope_weight, rope_weight_v),
                (query_rope, query_rope_v),
                (query_latent, query_v),
                (expert_ids, ids_v),
                (value_weight, value_v),
                (out_weight, out_v),
                (mixer_gain, mixer_gain_v),
                (group_router, group_router_v),
                (expert_router, expert_router_v),
            ]
        )
    ]
    caches = [
        pltpu.make_async_copy(cache_latent.at[s], cache_v.at[s], cache_sem.at[s])
        for s in range(seqs)
    ]
    ropes = [
        pltpu.make_async_copy(cache_rope.at[s], rope_v.at[s], rope_sem.at[s])
        for s in range(seqs)
    ]
    expert_loads = [
        [
            pltpu.make_async_copy(src.at[l], dst.at[l], expert_sem.at[k, l])
            for l in range(local_experts)
        ]
        for k, (src, dst) in enumerate(
            [(gate_weight, gate_v), (up_weight, up_v), (down_weight, down_v)]
        )
    ]
    length_load = pltpu.make_async_copy(lengths_hbm, lengths, length_sem)
    length_load.start()
    for load in loads[:8]:
        load.start()
    for s in range(seqs):
        ropes[s].start()
        caches[s].start()
    for load in loads[8:]:
        load.start()

    barrier = pltpu.get_barrier_semaphore()

    def greet(e, t):
        pl.semaphore_signal(
            barrier,
            inc=1,
            device_id={"ep": e, "tp": t},
            device_id_type=pl.DeviceIdType.MESH,
        )

    def greet_core(i, carry):
        to = lax.rem(my_chip + i, n_chip)
        greet(to // n_z, 2 * lax.rem(to, n_z) + core)
        return carry

    lax.fori_loop(1, n_chip, greet_core, 0)
    for k in range(n_z):
        greet(my_e, 2 * k + 1 - core)

    def remote(src, dst, send_sem, recv_sem, e, t):
        return pltpu.make_async_remote_copy(
            src_ref=src,
            dst_ref=dst,
            send_sem=send_sem,
            recv_sem=recv_sem,
            device_id={"ep": e, "tp": t},
            device_id_type=pl.DeviceIdType.MESH,
        )

    length_load.wait()
    ropes[0].wait()
    caches[0].wait()
    for i in (0, 1, 2, 3, 4, 5, 6):
        loads[i].wait()
    resid = residual_v[...].astype(F32)
    gain = norm_gain_v[...].astype(F32).reshape(1, width)
    normed_all = (resid * inverse_rms(resid) * gain).astype(BF16)
    own = jnp.where(
        iota((seqs, rows), 1) == my_t * seqs + iota((seqs, rows), 0), 1.0, 0.0
    ).astype(BF16)
    normed = dot(own, normed_all).astype(BF16)
    latent_raw = dot(normed, latent_weight_v[...])
    new_latent = (
        latent_raw * inverse_rms(latent_raw) * latent_gain_v[...].astype(F32).reshape(1, latent)
    ).astype(BF16)
    position = jnp.zeros((seqs, 1), F32)
    for s in range(seqs):
        position = jnp.where(iota((seqs, 1), 0) == s, lengths[s].astype(F32), position)
    index = iota((1, rope_width), 1)
    index = jnp.where(index >= half, index - half, index).astype(F32)
    frequency = jnp.power(jnp.full((1, rope_width), ROPE_BASE, F32), -2.0 * index / rope_width)
    angles = position * frequency
    cosine = jnp.cos(angles)
    sine = jnp.sin(angles)
    weight_r = rope_weight_v[...]
    swapped = jnp.concatenate([-weight_r[half:], weight_r[:half]], axis=0)
    new_rope = (
        dot(normed, weight_r, ((1,), (1,))) * cosine + dot(normed, swapped, ((1,), (1,))) * sine
    ).astype(BF16)
    latent_v[...] = new_latent
    rope_key_v[...] = new_rope
    stores = [
        pltpu.make_async_copy(latent_v, latent_out, store_sem.at[n_tp]),
        pltpu.make_async_copy(rope_key_v, rope_out, store_sem.at[n_tp + 1]),
    ]
    for store in stores:
        store.start()
    source = iota((rope_width, rope_width), 0)
    target = iota((rope_width, rope_width), 1)
    turn = (
        jnp.where(source + half == target, 1.0, 0.0) - jnp.where(source == target + half, 1.0, 0.0)
    ).astype(BF16)

    new_latent_f = new_latent.astype(F32)
    new_rope_f = new_rope.astype(F32)

    def scores(s):
        query = query_v[s]
        query_r = query_rope_v[s]
        turned = (
            query_r.astype(F32) * cosine[s : s + 1] + dot(query_r, turn) * sine[s : s + 1]
        ).astype(BF16)
        fresh = (
            jnp.sum(query.astype(F32) * new_latent_f[s : s + 1], axis=1, keepdims=True)
            + jnp.sum(turned.astype(F32) * new_rope_f[s : s + 1], axis=1, keepdims=True)
        ) * scale
        score = (dot(query, cache_v[s], ((1,), (1,))) + dot(turned, rope_v[s])) * scale
        score = jnp.where(iota((heads, length), 1) < lengths[s], score, -jnp.inf)
        return score, fresh

    def mix(s, score, fresh):
        top = jnp.maximum(jnp.max(score, axis=1, keepdims=True), fresh)
        powers = jnp.exp(score - top)
        fresh_power = jnp.exp(fresh - top)
        inverse = 1.0 / (jnp.sum(powers, axis=1, keepdims=True) + fresh_power)
        weight = (powers * inverse).astype(BF16)
        fresh_weight = (fresh_power * inverse).astype(BF16).astype(F32)
        return (dot(weight, cache_v[s]) + fresh_weight * new_latent_f[s : s + 1]).astype(BF16)

    mixed_latents = []
    waiting = None
    for s in range(seqs):
        if s > 0:
            ropes[s].wait()
            caches[s].wait()
        if s == seqs - 1:
            for kind in expert_loads:
                for load in kind:
                    load.start()
        found = scores(s)
        if waiting is not None:
            mixed_latents.append(mix(s - 1, *waiting))
        waiting = found
    mixed_latents.append(mix(seqs - 1, *waiting))
    lhs = jnp.concatenate(mixed_latents, axis=0)

    loads[8].wait()
    for t in range(n_tp):
        found = dot(lhs, value_v[:, t * head_cols : (t + 1) * head_cols])
        head = iota((heads, head_cols), 0)
        column = iota((heads, head_cols), 1) + t * head_cols
        mine = (column >= head * value_dim) & (column < (head + 1) * value_dim)
        block = jnp.zeros((pad, head_cols), F32)
        for s in range(seqs):
            line = jnp.sum(
                jnp.where(mine, found[s * heads : (s + 1) * heads], 0.0), axis=0, keepdims=True
            )
            block = jnp.where(iota((pad, head_cols), 0) == s, line, block)
        head_send[t] = block.astype(BF16)
    pl.semaphore_wait(barrier, n_chip - 1 + n_z)
    for i in range(1, n_tp):
        t = lax.rem(my_t + i, n_tp)
        remote(
            head_send.at[t], head_recv.at[my_t], head_sems.at[0, t], head_sems.at[1, my_t], my_e, t
        ).start()
    loads[7].wait()
    id0 = ids_v[0:1, :]
    id1 = ids_v[1:2, :]
    low = iota((n_ep, rows), 0) * local_experts
    high = low + local_experts
    hits = jnp.where(
        ((id0 >= low) & (id0 < high)) | ((id1 >= low) & (id1 < high)), 1.0, 0.0
    ).astype(F32)
    before = jnp.where(iota((rows, rows), 0) < iota((rows, rows), 1), 1.0, 0.0).astype(BF16)
    rank = dot(hits.astype(BF16), before)
    slot_of = jnp.where(hits > 0.5, rank, -1.0)
    slot_row = iota((slots, rows), 0).astype(F32)
    select = jnp.concatenate(
        [jnp.where(slot_row == slot_of[d : d + 1, :], 1.0, 0.0).astype(F32) for d in range(n_ep)],
        axis=0,
    )
    tag0 = jnp.sum(select * (id0.astype(F32) + 1.0), axis=1, keepdims=True)
    tag1 = jnp.sum(select * (id1.astype(F32) + 1.0), axis=1, keepdims=True)
    lane = iota((n_ep * slots, 128), 1)
    tags = jnp.where(lane == 0, tag0, jnp.where(lane == 1, tag1, 0.0))
    for d in range(n_ep):
        meta_send[d] = tags[d * slots : (d + 1) * slots]
    meta_recv[my_e] = meta_send[my_e]
    select_b = select.astype(BF16)

    for i in range(1, n_ep):
        e = lax.rem(my_e + i, n_ep)
        remote(
            meta_send.at[e], meta_recv.at[my_e], meta_sems.at[0, e], meta_sems.at[1, my_e], e, my_t
        ).start()
    head_recv[my_t] = head_send[my_t]
    loads[9].wait()
    line = iota((rows, n_tp * pad), 0)
    spot = iota((rows, n_tp * pad), 1)
    inner = spot & (pad - 1)
    outer = lax.shift_right_logical(spot, pad.bit_length() - 1)
    gather = jnp.where((inner < seqs) & (line == outer * seqs + inner), 1.0, 0.0).astype(BF16)
    for i in range(1, n_tp):
        t = lax.rem(my_t + i, n_tp)
        remote(
            head_send.at[t], head_recv.at[t], head_sems.at[0, t], head_sems.at[1, t], my_e, t
        ).wait()
    by_heads = dot(
        gather, head_recv[...].astype(F32).reshape(n_tp * pad, head_cols).astype(BF16)
    ).astype(BF16)

    def half(send, recv, sems, k):
        return remote(send.at[k], recv.at[k], sems.at[0, k], sems.at[1, k], my_e, sibling)

    def columns(t):
        return pl.ds(pl.multiple_of(t * col, col), col)

    for i in range(1, n_z + 1):
        k = lax.rem(my_z + i, n_z)
        half_send[k] = dot(by_heads, out_v[:, columns(2 * k + 1 - core)]).astype(BF16)
        half(half_send, half_recv, half_sems, k).start()
    for i in range(1, n_z + 1):
        k = lax.rem(my_z + i, n_z)
        t = 2 * k + core
        part = dot(by_heads, out_v[:, columns(t)])
        half(half_send, half_recv, half_sems, k).wait()
        attended = part + half_recv[k].astype(F32)
        if i < n_z:
            sum_send[k] = attended.astype(BF16)
            remote(
                sum_send.at[k], sum_recv.at[my_z], sum_sems.at[0, k], sum_sems.at[1, my_z], my_e, t
            ).start()
    my_cols = columns(my_t)
    for i in range(1, n_z):
        k = lax.rem(my_z + n_z - i, n_z)
        remote(
            sum_send.at[k],
            sum_recv.at[k],
            sum_sems.at[0, k],
            sum_sems.at[1, k],
            my_e,
            2 * k + core,
        ).wait()
        attended = attended + sum_recv[k].astype(F32)
    after = (residual_v[:, my_cols].astype(F32) + attended).astype(BF16)

    chosen = dot(select_b, after).astype(BF16)
    for d in range(n_ep):
        disp_send[d] = chosen[d * slots : (d + 1) * slots]
    disp_recv[my_e, my_t] = disp_send[my_e]

    def send_rows(i, carry):
        to = lax.rem(my_chip + i, n_chip)
        e = to // n_z
        k = lax.rem(to, n_z)
        remote(
            disp_send.at[e],
            disp_recv.at[my_e, my_t],
            disp_sems.at[0, e, k],
            disp_sems.at[1, my_e, my_z],
            e,
            2 * k + core,
        ).start()
        return carry

    lax.fori_loop(1, n_chip, send_rows, 0)
    remote(
        disp_send.at[my_e],
        disp_recv.at[my_e, my_t],
        pass_sems.at[0, my_e, my_z],
        pass_sems.at[1, my_e, my_z],
        my_e,
        sibling,
    ).start()
    for load in loads[10:13]:
        load.wait()

    def pass_rows(e, k):
        return remote(
            disp_recv.at[e, 2 * k + core],
            disp_recv.at[e, 2 * k + core],
            pass_sems.at[0, e, k],
            pass_sems.at[1, e, k],
            my_e,
            sibling,
        )

    def await_rows(i, carry):
        to = lax.rem(my_chip + n_chip - i, n_chip)
        e = to // n_z
        k = lax.rem(to, n_z)
        remote(
            disp_send.at[e],
            disp_recv.at[e, 2 * k + core],
            disp_sems.at[0, e, k],
            disp_sems.at[1, e, k],
            e,
            2 * k + core,
        ).wait()
        pass_rows(e, k).start()
        return carry

    def await_passed(i, carry):
        to = lax.rem(my_chip + n_chip - i, n_chip)
        pass_rows(to // n_z, lax.rem(to, n_z)).wait()
        return carry

    for i in range(1, n_ep):
        e = lax.rem(my_e + i, n_ep)
        remote(
            meta_send.at[e], meta_recv.at[e], meta_sems.at[0, e], meta_sems.at[1, e], e, my_t
        ).wait()
    lax.fori_loop(1, n_chip, await_rows, 0)
    lax.fori_loop(0, n_chip, await_passed, 0)
    total = n_ep * slots
    taken = jnp.concatenate(
        [disp_recv[:, t].reshape(total, col) for t in range(n_tp)], axis=1
    ).astype(F32)
    mixer = mixer_gain_v[...].astype(F32).reshape(1, width)
    expert_in = (taken * inverse_rms(taken) * mixer).astype(BF16)
    group_logits = dot(expert_in, group_router_v[...], ((1,), (1,)))
    expert_logits = dot(expert_in, expert_router_v[...], ((1,), (1,)))
    meta = meta_recv[...].reshape(total, 128)
    name0 = meta[:, 0:1] - 1.0
    name1 = meta[:, 1:2] - 1.0
    group_low = (iota((total, groups), 1) * per_group).astype(F32)
    in_group = (name0 >= group_low) & (name0 < group_low + per_group)
    group_top = jnp.sum(jnp.where(in_group, group_logits, 0.0), axis=1, keepdims=True)
    share = 1.0 / jnp.sum(jnp.exp(group_logits - group_top), axis=1, keepdims=True)
    number = iota((total, experts), 1).astype(F32)
    pick0 = jnp.sum(jnp.where(number == name0, expert_logits, 0.0), axis=1, keepdims=True)
    pick1 = jnp.sum(jnp.where(number == name1, expert_logits, 0.0), axis=1, keepdims=True)
    route0 = share / (1.0 + jnp.exp(pick1 - pick0))
    route1 = share / (1.0 + jnp.exp(pick0 - pick1))

    acts = []
    routes = []
    for l in range(local_experts):
        name = (my_e * local_experts + l).astype(F32)
        routes.append(
            jnp.where(name0 == name, route0, 0.0) + jnp.where(name1 == name, route1, 0.0)
        )
        expert_loads[0][l].wait()
        gate = dot(expert_in, gate_v[l])
        expert_loads[1][l].wait()
        up = dot(expert_in, up_v[l])
        acts.append((gate / (1.0 + jnp.exp(-gate)) * up).astype(BF16))
    for load in expert_loads[2]:
        load.wait()
    def expert_part(t):
        part = routes[0] * dot(acts[0], down_v[0, :, columns(t)])
        for l in range(1, local_experts):
            part = part + routes[l] * dot(acts[l], down_v[l, :, columns(t)])
        return part

    for i in range(1, n_z + 1):
        k = lax.rem(my_z + i, n_z)
        pair_send[k] = expert_part(2 * k + 1 - core).astype(BF16)
        half(pair_send, pair_recv, pair_sems, k).start()
    for i in range(1, n_z + 1):
        k = lax.rem(my_z + i, n_z)
        t = 2 * k + core
        part = expert_part(t)
        half(pair_send, pair_recv, pair_sems, k).wait()
        part = (part + pair_recv[k].astype(F32)).astype(BF16)
        for e in range(n_ep):
            ret_send[e, k] = part[e * slots : (e + 1) * slots]
        for d in range(1 if i == n_z else 0, n_ep):
            e = lax.rem(my_e + d, n_ep)
            remote(
                ret_send.at[e, k],
                ret_recv.at[my_e, my_z],
                ret_sems.at[0, e, k],
                ret_sems.at[1, my_e, my_z],
                e,
                t,
            ).start()
    ret_recv[my_e, my_z] = ret_send[my_e, my_z]

    def await_sums(i, carry):
        to = lax.rem(my_chip + n_chip - i, n_chip)
        e = to // n_z
        k = lax.rem(to, n_z)
        remote(
            ret_send.at[e, k],
            ret_recv.at[e, k],
            ret_sems.at[0, e, k],
            ret_sems.at[1, e, k],
            e,
            2 * k + core,
        ).wait()
        return carry

    lax.fori_loop(1, n_chip, await_sums, 0)
    gathered = ret_recv[:, 0].astype(F32)
    for t in range(1, n_z):
        gathered = gathered + ret_recv[:, t].astype(F32)
    moe = dot(
        select, gathered.reshape(total, col), ((0,), (0,)), precision=lax.Precision.HIGHEST
    )
    share_send[...] = (after.astype(F32) + moe).astype(BF16)
    for i in range(1, n_tp):
        t = lax.rem(my_t + i, n_tp)
        remote(
            share_send, share_recv.at[my_t], share_sems.at[0, t], share_sems.at[1, my_t], my_e, t
        ).start()

    def store(src, t):
        return pltpu.make_async_copy(src, mixed_out.at[:, columns(t)], store_sem.at[t])

    store(share_send, my_t).start()
    for i in range(1, n_tp):
        t = lax.rem(my_t + n_tp - i, n_tp)
        remote(
            share_send, share_recv.at[t], share_sems.at[0, t], share_sems.at[1, t], my_e, t
        ).wait()
        store(share_recv.at[t], t).start()
    for k in range(n_tp):
        store(share_send, k).wait()
    for copy in stores:
        copy.wait()


def place(arrays):
    def kernel(*refs):
        for src, dst in zip(refs[: len(arrays)], refs[len(arrays) :]):
            dst[...] = src[...]

    vmem = pl.BlockSpec(memory_space=pltpu.VMEM)
    return pl.pallas_call(
        kernel,
        out_shape=tuple(jax.ShapeDtypeStruct(a.shape, a.dtype) for a in arrays),
        in_specs=[vmem] * len(arrays),
        out_specs=(vmem,) * len(arrays),
        name="place",
    )(*arrays)


def on_device(n_ep, n_tp, *args):
    (
        residual,
        cache_latent,
        cache_rope,
        lengths,
        query_latent,
        query_rope,
        norm_gain,
        latent_weight,
        latent_gain,
        rope_weight,
        value_weight,
        out_weight,
        mixer_gain,
        group_router,
        expert_router,
        expert_ids,
        gate_weight,
        up_weight,
        down_weight,
    ) = args
    rows, width = residual.shape
    seqs, heads, latent = query_latent.shape
    rope_width = query_rope.shape[2]
    local_experts = gate_weight.shape[0]
    experts = expert_router.shape[1]
    per_group = experts // group_router.shape[1]
    capacity = 2 * rows * TOPK // experts
    slots = capacity if per_group == TOPK == local_experts else min(local_experts * capacity, rows)
    slots = -(-slots // 16) * 16
    col = width // n_tp
    n_z = n_tp // 2
    head_cols = out_weight.shape[0]
    pad = 8
    while pad < seqs:
        pad *= 2
    value_dim = value_weight.shape[1] // heads
    scale = float((value_dim + rope_width) ** (-0.5))
    group_router = group_router.T
    expert_router = expert_router.T
    expert_ids = expert_ids.T
    hbm = pl.BlockSpec(memory_space=pl.ANY)

    def held(array):
        return pltpu.VMEM(array.shape, array.dtype)

    dma = pltpu.SemaphoreType.DMA
    outs = pl.pallas_call(
        functools.partial(layer, (n_ep, n_tp, slots, scale)),
        out_shape=(
            jax.ShapeDtypeStruct((rows, width), BF16),
            jax.ShapeDtypeStruct((seqs, latent), BF16),
            jax.ShapeDtypeStruct((seqs, rope_width), BF16),
        ),
        in_specs=[hbm] * 19,
        out_specs=(hbm, hbm, hbm),
        scratch_shapes=[
            pltpu.SMEM(lengths.shape, lengths.dtype),
            held(residual),
            held(cache_latent),
            held(cache_rope),
            held(query_latent),
            held(query_rope),
            held(norm_gain),
            held(latent_weight),
            held(latent_gain),
            held(rope_weight),
            held(value_weight),
            held(out_weight),
            held(mixer_gain),
            held(group_router),
            held(expert_router),
            held(expert_ids),
            held(gate_weight),
            held(up_weight),
            held(down_weight),
            pltpu.VMEM((n_tp, pad, head_cols), BF16),
            pltpu.VMEM((n_tp, pad, head_cols), BF16),
            pltpu.VMEM((n_ep, slots, 128), F32),
            pltpu.VMEM((n_ep, slots, 128), F32),
            pltpu.VMEM((n_z, rows, col), BF16),
            pltpu.VMEM((n_z, rows, col), BF16),
            pltpu.VMEM((n_z, rows, col), BF16),
            pltpu.VMEM((n_z, rows, col), BF16),
            pltpu.VMEM((n_ep, slots, col), BF16),
            pltpu.VMEM((n_ep, n_tp, slots, col), BF16),
            pltpu.VMEM((n_z, n_ep * slots, col), BF16),
            pltpu.VMEM((n_z, n_ep * slots, col), BF16),
            pltpu.VMEM((n_ep, n_z, slots, col), BF16),
            pltpu.VMEM((n_ep, n_z, slots, col), BF16),
            pltpu.VMEM((rows, col), BF16),
            pltpu.VMEM((n_tp, rows, col), BF16),
            pltpu.VMEM((seqs, latent), BF16),
            pltpu.VMEM((seqs, rope_width), BF16),
            dma,
            dma((13,)),
            dma((seqs,)),
            dma((seqs,)),
            dma((3, local_experts)),
            dma((2, n_tp)),
            dma((2, n_ep)),
            dma((2, n_z)),
            dma((2, n_z)),
            dma((2, n_ep, n_z)),
            dma((2, n_ep, n_z)),
            dma((2, n_z)),
            dma((2, n_ep, n_z)),
            dma((2, n_tp)),
            dma((n_tp + 2,)),
        ],
        compiler_params=pltpu.CompilerParams(collective_id=0, has_side_effects=True),
        name="layer",
    )(
        residual,
        cache_latent,
        cache_rope,
        lengths,
        query_latent,
        query_rope,
        norm_gain,
        latent_weight,
        latent_gain,
        rope_weight,
        value_weight,
        out_weight,
        mixer_gain,
        group_router,
        expert_router,
        expert_ids,
        gate_weight,
        up_weight,
        down_weight,
    )
    return place(outs)


def solution(mesh):
    in_specs = (
        P("ep", None),
        P(("ep", "tp"), None, None),
        P(("ep", "tp"), None, None),
        P(("ep", "tp")),
        P(("ep", "tp"), None, None),
        P(("ep", "tp"), None, None),
        P(),
        P(),
        P(),
        P(),
        P(),
        P("tp", None),
        P(),
        P(),
        P(),
        P("ep", None),
        P("ep", None, "tp"),
        P("ep", None, "tp"),
        P("ep", "tp", None),
    )
    out_specs = (P("ep", None), P(("ep", "tp"), None), P(("ep", "tp"), None))
    return jax.shard_map(
        functools.partial(on_device, mesh.shape["ep"], mesh.shape["tp"]),
        mesh=mesh,
        in_specs=in_specs,
        out_specs=out_specs,
        check_vma=False,
    )
```

```python
import functools

import jax
import jax.numpy as jnp
from jax import lax
from jax.experimental import pallas as pl
from jax.experimental.pallas import tpu as pltpu
from jax.sharding import PartitionSpec as P

NORM_EPSILON = 1e-06
ROPE_BASE = 10000.0
TOPK = 2

F32 = jnp.float32
BF16 = jnp.bfloat16


def dot(a, b, contract=((1,), (0,)), precision=None):
    return lax.dot_general(
        a, b, (contract, ((), ())), preferred_element_type=F32, precision=precision
    )


def inverse_rms(values):
    return lax.rsqrt(jnp.mean(values * values, axis=-1, keepdims=True) + NORM_EPSILON)


def iota(shape, dim):
    return lax.broadcasted_iota(jnp.int32, shape, dim)


def layer(
    sizes,
    residual,
    cache_latent,
    cache_rope,
    lengths_hbm,
    query_latent,
    query_rope,
    norm_gain,
    latent_weight,
    latent_gain,
    rope_weight,
    value_weight,
    out_weight,
    mixer_gain,
    group_router,
    expert_router,
    expert_ids,
    gate_weight,
    up_weight,
    down_weight,
    mixed_out,
    latent_out,
    rope_out,
    lengths,
    residual_v,
    cache_v,
    rope_v,
    query_v,
    query_rope_v,
    norm_gain_v,
    latent_weight_v,
    latent_gain_v,
    rope_weight_v,
    value_v,
    out_v,
    mixer_gain_v,
    group_router_v,
    expert_router_v,
    ids_v,
    gate_v,
    up_v,
    down_v,
    head_send,
    head_recv,
    meta_send,
    meta_recv,
    half_send,
    half_recv,
    sum_send,
    sum_recv,
    disp_send,
    disp_recv,
    pair_send,
    pair_recv,
    ret_send,
    ret_recv,
    share_send,
    gain_row,
    length_sem,
    load_sem,
    cache_sem,
    rope_sem,
    expert_sem,
    head_sems,
    meta_sems,
    half_sems,
    sum_sems,
    disp_sems,
    pass_sems,
    pair_sems,
    ret_sems,
    share_sems,
    store_sem,
):
    n_ep, n_tp, slots, scale = sizes
    rows, width = residual_v.shape
    seqs, heads, latent = query_v.shape
    rope_width = rope_weight_v.shape[0]
    half = rope_width // 2
    length = cache_v.shape[1]
    pad = head_send.shape[1]
    head_cols = head_send.shape[2]
    col = width // n_tp
    local_experts = gate_v.shape[0]
    experts = expert_router_v.shape[0]
    groups = group_router_v.shape[0]
    per_group = experts // groups
    value_dim = value_v.shape[1] // heads

    my_e = lax.axis_index("ep")
    my_t = lax.axis_index("tp")
    n_z = n_tp // 2
    my_z = my_t // 2
    core = lax.rem(my_t, 2)
    sibling = my_t + 1 - 2 * core
    n_chip = n_ep * n_z
    my_chip = my_e * n_z + my_z

    loads = [
        pltpu.make_async_copy(src, dst, load_sem.at[i])
        for i, (src, dst) in enumerate(
            [
                (residual, residual_v),
                (norm_gain, norm_gain_v),
                (latent_weight, latent_weight_v),
                (latent_gain, latent_gain_v),
                (rope_weight, rope_weight_v),
                (query_rope, query_rope_v),
                (query_latent, query_v),
                (expert_ids, ids_v),
                (value_weight, value_v),
                (out_weight, out_v),
                (mixer_gain, mixer_gain_v),
                (group_router, group_router_v),
                (expert_router, expert_router_v),
            ]
        )
    ]
    caches = [
        pltpu.make_async_copy(cache_latent.at[s], cache_v.at[s], cache_sem.at[s])
        for s in range(seqs)
    ]
    ropes = [
        pltpu.make_async_copy(cache_rope.at[s], rope_v.at[s], rope_sem.at[s])
        for s in range(seqs)
    ]
    expert_loads = [
        [
            pltpu.make_async_copy(src.at[l], dst.at[l], expert_sem.at[k, l])
            for l in range(local_experts)
        ]
        for k, (src, dst) in enumerate(
            [(gate_weight, gate_v), (up_weight, up_v), (down_weight, down_v)]
        )
    ]
    length_load = pltpu.make_async_copy(lengths_hbm, lengths, length_sem)
    length_load.start()
    for i in (5, 6):
        loads[i].start()
    for s in range(seqs):
        ropes[s].start()
        caches[s].start()
        if s == 0:
            for i in (0, 1, 2, 3, 4):
                loads[i].start()
    for load in loads[7:]:
        load.start()

    barrier = pltpu.get_barrier_semaphore()

    def flip(index, by, count):
        found = 0
        bit = 1
        while bit < count:
            found = found + bit * lax.rem(index // bit + by // bit, 2)
            bit *= 2
        return found

    near_z = [flip(my_z, i, n_z) for i in range(n_z)]
    near_e = [flip(my_e, i, n_ep) for i in range(n_ep)]
    far_first = near_z[::-1]

    def greet(e, t):
        pl.semaphore_signal(
            barrier,
            inc=1,
            device_id={"ep": e, "tp": t},
            device_id_type=pl.DeviceIdType.MESH,
        )

    def greet_core(i, carry):
        to = lax.rem(my_chip + i, n_chip)
        greet(to // n_z, 2 * lax.rem(to, n_z) + core)
        return carry

    lax.fori_loop(1, n_chip, greet_core, 0)
    for k in range(n_z):
        greet(my_e, 2 * k + 1 - core)

    def remote(src, dst, send_sem, recv_sem, e, t):
        return pltpu.make_async_remote_copy(
            src_ref=src,
            dst_ref=dst,
            send_sem=send_sem,
            recv_sem=recv_sem,
            device_id={"ep": e, "tp": t},
            device_id_type=pl.DeviceIdType.MESH,
        )

    length_load.wait()
    position = jnp.zeros((seqs, 1), F32)
    for s in range(seqs):
        position = jnp.where(iota((seqs, 1), 0) == s, lengths[s].astype(F32), position)
    index = iota((1, rope_width), 1)
    index = jnp.where(index >= half, index - half, index).astype(F32)
    frequency = jnp.power(jnp.full((1, rope_width), ROPE_BASE, F32), -2.0 * index / rope_width)
    angles = position * frequency
    cosine = jnp.cos(angles)
    sine = jnp.sin(angles)
    source = iota((rope_width, rope_width), 0)
    target = iota((rope_width, rope_width), 1)
    turn = (
        jnp.where(source + half == target, 1.0, 0.0) - jnp.where(source == target + half, 1.0, 0.0)
    ).astype(BF16)


    def scores(s):
        query_r = query_rope_v[s]
        turned = (
            query_r.astype(F32) * cosine[s : s + 1] + dot(query_r, turn) * sine[s : s + 1]
        ).astype(BF16)
        score = (dot(query_v[s], cache_v[s], ((1,), (1,))) + dot(turned, rope_v[s])) * scale
        score = jnp.where(iota((heads, length), 1) < lengths[s], score, -jnp.inf)
        return score, turned

    for i in (5, 6):
        loads[i].wait()
    ropes[0].wait()
    caches[0].wait()
    waiting = scores(0)

    for i in (0, 1, 2, 3, 4):
        loads[i].wait()
    resid = residual_v[...].astype(F32)
    gain = norm_gain_v[...].astype(F32).reshape(1, width)
    normed_all = (resid * inverse_rms(resid) * gain).astype(BF16)
    own = jnp.where(
        iota((seqs, rows), 1) == my_t * seqs + iota((seqs, rows), 0), 1.0, 0.0
    ).astype(BF16)
    normed = dot(own, normed_all).astype(BF16)
    latent_raw = dot(normed, latent_weight_v[...])
    new_latent = (
        latent_raw * inverse_rms(latent_raw) * latent_gain_v[...].astype(F32).reshape(1, latent)
    ).astype(BF16)
    weight_r = rope_weight_v[...]
    swapped = jnp.concatenate([-weight_r[half:], weight_r[:half]], axis=0)
    new_rope = (
        dot(normed, weight_r, ((1,), (1,))) * cosine + dot(normed, swapped, ((1,), (1,))) * sine
    ).astype(BF16)
    latent_out[...] = new_latent
    rope_out[...] = new_rope
    new_latent_f = new_latent.astype(F32)
    new_rope_f = new_rope.astype(F32)

    def mix(s, score, turned):
        fresh = (
            jnp.sum(query_v[s].astype(F32) * new_latent_f[s : s + 1], axis=1, keepdims=True)
            + jnp.sum(turned.astype(F32) * new_rope_f[s : s + 1], axis=1, keepdims=True)
        ) * scale
        top = jnp.maximum(jnp.max(score, axis=1, keepdims=True), fresh)
        powers = jnp.exp(score - top)
        fresh_power = jnp.exp(fresh - top)
        inverse = 1.0 / (jnp.sum(powers, axis=1, keepdims=True) + fresh_power)
        fresh_weight = fresh_power.astype(BF16).astype(F32)
        mixed = dot(powers.astype(BF16), cache_v[s]) + fresh_weight * new_latent_f[s : s + 1]
        return (mixed * inverse).astype(BF16)

    mixed_latents = []
    for s in range(1, seqs):
        ropes[s].wait()
        caches[s].wait()
        if s == seqs - 1:
            for kind in expert_loads:
                for load in kind:
                    load.start()
        found = scores(s)
        mixed_latents.append(mix(s - 1, *waiting))
        waiting = found
    mixed_latents.append(mix(seqs - 1, *waiting))
    lhs = jnp.concatenate(mixed_latents, axis=0)

    loads[8].wait()
    for t in range(n_tp):
        found = dot(lhs, value_v[:, t * head_cols : (t + 1) * head_cols])
        head = iota((heads, head_cols), 0)
        column = iota((heads, head_cols), 1) + t * head_cols
        mine = (column >= head * value_dim) & (column < (head + 1) * value_dim)
        block = jnp.zeros((pad, head_cols), F32)
        for s in range(seqs):
            line = jnp.sum(
                jnp.where(mine, found[s * heads : (s + 1) * heads], 0.0), axis=0, keepdims=True
            )
            block = jnp.where(iota((pad, head_cols), 0) == s, line, block)
        head_send[t] = block.astype(BF16)
    pl.semaphore_wait(barrier, n_chip - 1 + n_z)
    for i in reversed(range(1, n_tp)):
        t = flip(my_t, i, n_tp)
        remote(
            head_send.at[t], head_recv.at[my_t], head_sems.at[0, t], head_sems.at[1, my_t], my_e, t
        ).start()
    loads[7].wait()
    id0 = ids_v[0:1, :]
    id1 = ids_v[1:2, :]
    low = iota((n_ep, rows), 0) * local_experts
    high = low + local_experts
    hits = jnp.where(
        ((id0 >= low) & (id0 < high)) | ((id1 >= low) & (id1 < high)), 1.0, 0.0
    ).astype(F32)
    before = jnp.where(iota((rows, rows), 0) < iota((rows, rows), 1), 1.0, 0.0).astype(BF16)
    rank = dot(hits.astype(BF16), before)
    slot_of = jnp.where(hits > 0.5, rank, -1.0)
    slot_row = iota((slots, rows), 0).astype(F32)
    select = jnp.concatenate(
        [jnp.where(slot_row == slot_of[d : d + 1, :], 1.0, 0.0).astype(F32) for d in range(n_ep)],
        axis=0,
    )
    tag0 = jnp.sum(select * (id0.astype(F32) + 1.0), axis=1, keepdims=True)
    tag1 = jnp.sum(select * (id1.astype(F32) + 1.0), axis=1, keepdims=True)
    lane = iota((n_ep * slots, 128), 1)
    tags = jnp.where(lane == 0, tag0, jnp.where(lane == 1, tag1, 0.0))
    for d in range(n_ep):
        meta_send[d] = tags[d * slots : (d + 1) * slots]
    meta_recv[my_e] = meta_send[my_e]
    select_b = select.astype(BF16)

    for i in range(1, n_ep):
        e = lax.rem(my_e + i, n_ep)
        remote(
            meta_send.at[e], meta_recv.at[my_e], meta_sems.at[0, e], meta_sems.at[1, my_e], e, my_t
        ).start()
    head_recv[my_t] = head_send[my_t]
    loads[9].wait()
    line = iota((rows, n_tp * pad), 0)
    spot = iota((rows, n_tp * pad), 1)
    inner = spot & (pad - 1)
    outer = lax.shift_right_logical(spot, pad.bit_length() - 1)
    gather = jnp.where((inner < seqs) & (line == outer * seqs + inner), 1.0, 0.0).astype(BF16)
    for i in range(1, n_tp):
        t = lax.rem(my_t + i, n_tp)
        remote(
            head_send.at[t], head_recv.at[t], head_sems.at[0, t], head_sems.at[1, t], my_e, t
        ).wait()
    by_heads = dot(
        gather, head_recv[...].astype(F32).reshape(n_tp * pad, head_cols).astype(BF16)
    ).astype(BF16)

    def half(send, recv, sems, k):
        return remote(send.at[k], recv.at[k], sems.at[0, k], sems.at[1, k], my_e, sibling)

    def columns(t):
        return pl.ds(pl.multiple_of(t * col, col), col)

    for k in far_first:
        half_send[k] = dot(by_heads, out_v[:, columns(2 * k + 1 - core)]).astype(BF16)
        half(half_send, half_recv, half_sems, k).start()
    parts = [dot(by_heads, out_v[:, columns(2 * k + core)]) for k in far_first]
    for i, k in enumerate(far_first):
        half(half_send, half_recv, half_sems, k).wait()
        attended = parts[i] + half_recv[k].astype(F32)
        if i < n_z - 1:
            sum_send[k] = attended.astype(BF16)
            remote(
                sum_send.at[k],
                sum_recv.at[my_z],
                sum_sems.at[0, k],
                sum_sems.at[1, my_z],
                my_e,
                2 * k + core,
            ).start()
    my_cols = columns(my_t)
    for k in reversed(far_first[:-1]):
        remote(
            sum_send.at[k],
            sum_recv.at[k],
            sum_sems.at[0, k],
            sum_sems.at[1, k],
            my_e,
            2 * k + core,
        ).wait()
        attended = attended + sum_recv[k].astype(F32)
    after = (residual_v[:, my_cols].astype(F32) + attended).astype(BF16)

    chosen = dot(select_b, after).astype(BF16)
    for d in range(n_ep):
        disp_send[d] = chosen[d * slots : (d + 1) * slots]
    disp_recv[my_e, my_t] = disp_send[my_e]

    for i in reversed(range(n_z)):
        for d in reversed(range(n_ep)):
            if i + d > 0:
                e, k = near_e[d], near_z[i]
                remote(
                    disp_send.at[e],
                    disp_recv.at[my_e, my_t],
                    disp_sems.at[0, e, k],
                    disp_sems.at[1, my_e, my_z],
                    e,
                    2 * k + core,
                ).start()
    remote(
        disp_send.at[my_e],
        disp_recv.at[my_e, my_t],
        pass_sems.at[0, my_e, my_z],
        pass_sems.at[1, my_e, my_z],
        my_e,
        sibling,
    ).start()
    for load in loads[10:13]:
        load.wait()

    def pass_rows(e, k):
        return remote(
            disp_recv.at[e, 2 * k + core],
            disp_recv.at[e, 2 * k + core],
            pass_sems.at[0, e, k],
            pass_sems.at[1, e, k],
            my_e,
            sibling,
        )

    def await_rows(i):
        for d in range(n_ep):
            if i + d > 0:
                e, k = near_e[d], near_z[i]
                remote(
                    disp_send.at[e],
                    disp_recv.at[e, 2 * k + core],
                    disp_sems.at[0, e, k],
                    disp_sems.at[1, e, k],
                    e,
                    2 * k + core,
                ).wait()
                pass_rows(e, k).start()

    for i in range(1, n_ep):
        e = near_e[i]
        remote(
            meta_send.at[e], meta_recv.at[e], meta_sems.at[0, e], meta_sems.at[1, e], e, my_t
        ).wait()
    for kind in expert_loads:
        for load in kind:
            load.wait()
    gain_row[...] = mixer_gain_v[...].astype(F32).reshape(1, width)
    total = n_ep * slots
    squares = jnp.zeros((total, 1), F32)
    group_logits = jnp.zeros((total, groups), F32)
    expert_logits = jnp.zeros((total, experts), F32)
    gates = [jnp.zeros((total, gate_v.shape[2]), F32) for _ in range(local_experts)]
    ups = [jnp.zeros((total, gate_v.shape[2]), F32) for _ in range(local_experts)]
    await_rows(0)
    for i in range(n_z):
        if i + 1 < n_z:
            await_rows(i + 1)
        k = near_z[i]
        for d in range(n_ep):
            pass_rows(near_e[d], k).wait()
        span = pl.ds(pl.multiple_of(2 * k * col, 2 * col), 2 * col)
        taken = jnp.concatenate(
            [disp_recv[:, 2 * k + h].reshape(total, col) for h in range(2)], axis=1
        ).astype(F32)
        squares = squares + jnp.sum(taken * taken, axis=1, keepdims=True)
        mixer = gain_row[:, span]
        scaled = (taken * mixer).astype(BF16)
        for l in range(local_experts):
            gates[l] = gates[l] + dot(scaled, gate_v[l, span, :])
            ups[l] = ups[l] + dot(scaled, up_v[l, span, :])
        group_logits = group_logits + dot(scaled, group_router_v[:, span], ((1,), (1,)))
        expert_logits = expert_logits + dot(scaled, expert_router_v[:, span], ((1,), (1,)))
    factor = lax.rsqrt(squares / width + NORM_EPSILON)
    group_logits = group_logits * factor
    expert_logits = expert_logits * factor
    meta = meta_recv[...].reshape(total, 128)
    name0 = meta[:, 0:1] - 1.0
    name1 = meta[:, 1:2] - 1.0
    group_low = (iota((total, groups), 1) * per_group).astype(F32)
    in_group = (name0 >= group_low) & (name0 < group_low + per_group)
    group_top = jnp.sum(jnp.where(in_group, group_logits, 0.0), axis=1, keepdims=True)
    share = 1.0 / jnp.sum(jnp.exp(group_logits - group_top), axis=1, keepdims=True)
    number = iota((total, experts), 1).astype(F32)
    pick0 = jnp.sum(jnp.where(number == name0, expert_logits, 0.0), axis=1, keepdims=True)
    pick1 = jnp.sum(jnp.where(number == name1, expert_logits, 0.0), axis=1, keepdims=True)
    route0 = share / (1.0 + jnp.exp(pick1 - pick0))
    route1 = share / (1.0 + jnp.exp(pick0 - pick1))

    acts = []
    routes = []
    for l in range(local_experts):
        name = (my_e * local_experts + l).astype(F32)
        routes.append(
            jnp.where(name0 == name, route0, 0.0) + jnp.where(name1 == name, route1, 0.0)
        )
        gate = gates[l] * factor
        acts.append((gate / (1.0 + jnp.exp(-gate)) * (ups[l] * factor)).astype(BF16))
    def expert_part(t):
        part = routes[0] * dot(acts[0], down_v[0, :, columns(t)])
        for l in range(1, local_experts):
            part = part + routes[l] * dot(acts[l], down_v[l, :, columns(t)])
        return part

    for k in far_first:
        pair_send[k] = expert_part(2 * k + 1 - core).astype(BF16)
        half(pair_send, pair_recv, pair_sems, k).start()
    for i, k in enumerate(far_first):
        t = 2 * k + core
        part = expert_part(t)
        half(pair_send, pair_recv, pair_sems, k).wait()
        part = (part + pair_recv[k].astype(F32)).astype(BF16)
        for e in range(n_ep):
            ret_send[e, k] = part[e * slots : (e + 1) * slots]
        for d in reversed(range(1 if i == n_z - 1 else 0, n_ep)):
            e = near_e[d]
            remote(
                ret_send.at[e, k],
                ret_recv.at[my_e, my_z],
                ret_sems.at[0, e, k],
                ret_sems.at[1, my_e, my_z],
                e,
                t,
            ).start()
    ret_recv[my_e, my_z] = ret_send[my_e, my_z]

    for i in range(n_z):
        for d in range(n_ep):
            if i + d > 0:
                e, k = near_e[d], near_z[i]
                remote(
                    ret_send.at[e, k],
                    ret_recv.at[e, k],
                    ret_sems.at[0, e, k],
                    ret_sems.at[1, e, k],
                    e,
                    2 * k + core,
                ).wait()
    gathered = ret_recv[:, 0].astype(F32)
    for t in range(1, n_z):
        gathered = gathered + ret_recv[:, t].astype(F32)
    gathered = gathered.reshape(total, col)
    coarse = gathered.astype(BF16)
    fine = (gathered - coarse.astype(F32)).astype(BF16)
    moe = dot(select_b, coarse, ((0,), (0,))) + dot(select_b, fine, ((0,), (0,)))
    share_send[...] = (after.astype(F32) + moe).astype(BF16)
    own_store = pltpu.make_async_copy(share_send, mixed_out.at[:, my_cols], store_sem)
    for i in reversed(range(1, n_tp)):
        t = flip(my_t, i, n_tp)
        remote(
            share_send,
            mixed_out.at[:, my_cols],
            share_sems.at[0, t],
            share_sems.at[1, my_t],
            my_e,
            t,
        ).start()
    own_store.start()
    for i in range(1, n_tp):
        t = flip(my_t, i, n_tp)
        remote(
            share_send,
            mixed_out.at[:, columns(t)],
            share_sems.at[0, t],
            share_sems.at[1, t],
            my_e,
            t,
        ).wait()
    own_store.wait()


def place(arrays):
    count = len(arrays)

    def kernel(*refs):
        copies = [
            pltpu.make_async_copy(refs[i], refs[count + i], refs[-1].at[i]) for i in range(count)
        ]
        for copy in copies:
            copy.start()
        for copy in copies:
            copy.wait()

    arrays = [pltpu.with_memory_space_constraint(a, pltpu.VMEM) for a in arrays]
    return pl.pallas_call(
        kernel,
        out_shape=tuple(jax.ShapeDtypeStruct(a.shape, a.dtype) for a in arrays),
        in_specs=[pl.BlockSpec(memory_space=pltpu.VMEM)] * count,
        out_specs=(pl.BlockSpec(memory_space=pl.ANY),) * count,
        scratch_shapes=[pltpu.SemaphoreType.DMA((count,))],
        name="place",
    )(*arrays)


def on_device(n_ep, n_tp, *args):
    (
        residual,
        cache_latent,
        cache_rope,
        lengths,
        query_latent,
        query_rope,
        norm_gain,
        latent_weight,
        latent_gain,
        rope_weight,
        value_weight,
        out_weight,
        mixer_gain,
        group_router,
        expert_router,
        expert_ids,
        gate_weight,
        up_weight,
        down_weight,
    ) = args
    rows, width = residual.shape
    seqs, heads, latent = query_latent.shape
    rope_width = query_rope.shape[2]
    local_experts = gate_weight.shape[0]
    experts = expert_router.shape[1]
    per_group = experts // group_router.shape[1]
    capacity = 2 * rows * TOPK // experts
    slots = capacity if per_group == TOPK == local_experts else min(local_experts * capacity, rows)
    slots = -(-slots // 16) * 16
    col = width // n_tp
    n_z = n_tp // 2
    head_cols = out_weight.shape[0]
    pad = 8
    while pad < seqs:
        pad *= 2
    value_dim = value_weight.shape[1] // heads
    scale = float((value_dim + rope_width) ** (-0.5))
    group_router = group_router.T
    expert_router = expert_router.T
    expert_ids = expert_ids.T
    hbm = pl.BlockSpec(memory_space=pl.ANY)

    def held(array):
        return pltpu.VMEM(array.shape, array.dtype)

    dma = pltpu.SemaphoreType.DMA
    outs = pl.pallas_call(
        functools.partial(layer, (n_ep, n_tp, slots, scale)),
        out_shape=(
            pltpu.VMEM((rows, width), BF16),
            pltpu.VMEM((seqs, latent), BF16),
            pltpu.VMEM((seqs, rope_width), BF16),
        ),
        in_specs=[hbm] * 19,
        out_specs=(pl.BlockSpec(memory_space=pltpu.VMEM),) * 3,
        scratch_shapes=[
            pltpu.SMEM(lengths.shape, lengths.dtype),
            held(residual),
            held(cache_latent),
            held(cache_rope),
            held(query_latent),
            held(query_rope),
            held(norm_gain),
            held(latent_weight),
            held(latent_gain),
            held(rope_weight),
            held(value_weight),
            held(out_weight),
            held(mixer_gain),
            held(group_router),
            held(expert_router),
            held(expert_ids),
            held(gate_weight),
            held(up_weight),
            held(down_weight),
            pltpu.VMEM((n_tp, pad, head_cols), BF16),
            pltpu.VMEM((n_tp, pad, head_cols), BF16),
            pltpu.VMEM((n_ep, slots, 128), F32),
            pltpu.VMEM((n_ep, slots, 128), F32),
            pltpu.VMEM((n_z, rows, col), BF16),
            pltpu.VMEM((n_z, rows, col), BF16),
            pltpu.VMEM((n_z, rows, col), BF16),
            pltpu.VMEM((n_z, rows, col), BF16),
            pltpu.VMEM((n_ep, slots, col), BF16),
            pltpu.VMEM((n_ep, n_tp, slots, col), BF16),
            pltpu.VMEM((n_z, n_ep * slots, col), BF16),
            pltpu.VMEM((n_z, n_ep * slots, col), BF16),
            pltpu.VMEM((n_ep, n_z, slots, col), BF16),
            pltpu.VMEM((n_ep, n_z, slots, col), BF16),
            pltpu.VMEM((rows, col), BF16),
            pltpu.VMEM((1, width), F32),
            dma,
            dma((13,)),
            dma((seqs,)),
            dma((seqs,)),
            dma((3, local_experts)),
            dma((2, n_tp)),
            dma((2, n_ep)),
            dma((2, n_z)),
            dma((2, n_z)),
            dma((2, n_ep, n_z)),
            dma((2, n_ep, n_z)),
            dma((2, n_z)),
            dma((2, n_ep, n_z)),
            dma((2, n_tp)),
            dma,
        ],
        compiler_params=pltpu.CompilerParams(collective_id=0, has_side_effects=True),
        name="layer",
    )(
        residual,
        cache_latent,
        cache_rope,
        lengths,
        query_latent,
        query_rope,
        norm_gain,
        latent_weight,
        latent_gain,
        rope_weight,
        value_weight,
        out_weight,
        mixer_gain,
        group_router,
        expert_router,
        expert_ids,
        gate_weight,
        up_weight,
        down_weight,
    )
    return place(outs)


def solution(mesh):
    in_specs = (
        P("ep", None),
        P(("ep", "tp"), None, None),
        P(("ep", "tp"), None, None),
        P(("ep", "tp")),
        P(("ep", "tp"), None, None),
        P(("ep", "tp"), None, None),
        P(),
        P(),
        P(),
        P(),
        P(),
        P("tp", None),
        P(),
        P(),
        P(),
        P("ep", None),
        P("ep", None, "tp"),
        P("ep", None, "tp"),
        P("ep", "tp", None),
    )
    out_specs = (P("ep", None), P(("ep", "tp"), None), P(("ep", "tp"), None))
    return jax.shard_map(
        functools.partial(on_device, mesh.shape["ep"], mesh.shape["tp"]),
        mesh=mesh,
        in_specs=in_specs,
        out_specs=out_specs,
        check_vma=False,
    )
```

```python
import functools

import jax
import jax.numpy as jnp
from jax import lax
from jax.experimental import pallas as pl
from jax.experimental.pallas import tpu as pltpu
from jax.sharding import PartitionSpec as P

NORM_EPSILON = 1e-06
ROPE_BASE = 10000.0
TOPK = 2

F32 = jnp.float32
BF16 = jnp.bfloat16


def dot(a, b, contract=((1,), (0,)), precision=None):
    return lax.dot_general(
        a, b, (contract, ((), ())), preferred_element_type=F32, precision=precision
    )


def inverse_rms(values):
    return lax.rsqrt(jnp.mean(values * values, axis=-1, keepdims=True) + NORM_EPSILON)


def iota(shape, dim):
    return lax.broadcasted_iota(jnp.int32, shape, dim)


def layer(
    sizes,
    residual,
    cache_latent,
    cache_rope,
    lengths_hbm,
    query_latent,
    query_rope,
    norm_gain,
    latent_weight,
    latent_gain,
    rope_weight,
    value_weight,
    out_weight,
    mixer_gain,
    group_router,
    expert_router,
    expert_ids,
    gate_weight,
    up_weight,
    down_weight,
    mixed_out,
    latent_out,
    rope_out,
    lengths,
    residual_v,
    cache_v,
    rope_v,
    query_v,
    query_rope_v,
    norm_gain_v,
    latent_weight_v,
    latent_gain_v,
    rope_weight_v,
    value_v,
    out_v,
    mixer_gain_v,
    group_router_v,
    expert_router_v,
    ids_v,
    gate_v,
    up_v,
    down_v,
    head_send,
    head_recv,
    meta_send,
    meta_recv,
    half_send,
    half_recv,
    sum_send,
    sum_recv,
    disp_send,
    disp_recv,
    pair_send,
    pair_recv,
    ret_send,
    ret_recv,
    share_send,
    gain_row,
    length_sem,
    load_sem,
    cache_sem,
    rope_sem,
    expert_sem,
    head_sems,
    meta_sems,
    half_sems,
    sum_sems,
    disp_sems,
    pass_sems,
    pair_sems,
    ret_sems,
    share_sems,
    store_sem,
):
    n_ep, n_tp, slots, scale = sizes
    rows, width = residual_v.shape
    seqs, heads, latent = query_v.shape
    rope_width = rope_weight_v.shape[0]
    half = rope_width // 2
    length = cache_v.shape[1]
    pad = head_send.shape[1]
    head_cols = head_send.shape[2]
    col = width // n_tp
    local_experts = gate_v.shape[0]
    experts = expert_router_v.shape[0]
    groups = group_router_v.shape[0]
    per_group = experts // groups
    value_dim = value_v.shape[1] // heads

    my_e = lax.axis_index("ep")
    my_t = lax.axis_index("tp")
    n_z = n_tp // 2
    my_z = my_t // 2
    core = lax.rem(my_t, 2)
    sibling = my_t + 1 - 2 * core
    n_chip = n_ep * n_z
    my_chip = my_e * n_z + my_z

    loads = [
        pltpu.make_async_copy(src, dst, load_sem.at[i])
        for i, (src, dst) in enumerate(
            [
                (residual, residual_v),
                (norm_gain, norm_gain_v),
                (latent_weight, latent_weight_v),
                (latent_gain, latent_gain_v),
                (rope_weight, rope_weight_v),
                (query_rope, query_rope_v),
                (query_latent, query_v),
                (expert_ids, ids_v),
                (value_weight, value_v),
                (out_weight, out_v),
                (mixer_gain, mixer_gain_v),
                (group_router, group_router_v),
                (expert_router, expert_router_v),
            ]
        )
    ]
    caches = [
        pltpu.make_async_copy(cache_latent.at[s], cache_v.at[s], cache_sem.at[s])
        for s in range(seqs)
    ]
    ropes = [
        pltpu.make_async_copy(cache_rope.at[s], rope_v.at[s], rope_sem.at[s])
        for s in range(seqs)
    ]
    expert_loads = [
        [
            pltpu.make_async_copy(src.at[l], dst.at[l], expert_sem.at[k, l])
            for l in range(local_experts)
        ]
        for k, (src, dst) in enumerate(
            [(gate_weight, gate_v), (up_weight, up_v), (down_weight, down_v)]
        )
    ]
    length_load = pltpu.make_async_copy(lengths_hbm, lengths, length_sem)
    length_load.start()
    for i in (5, 6):
        loads[i].start()
    for s in range(seqs):
        ropes[s].start()
        caches[s].start()
        if s == 0:
            for i in (0, 1, 2, 3, 4):
                loads[i].start()
    for load in loads[7:]:
        load.start()

    barrier = pltpu.get_barrier_semaphore()

    def flip(index, by, count):
        found = 0
        bit = 1
        while bit < count:
            found = found + bit * lax.rem(index // bit + by // bit, 2)
            bit *= 2
        return found

    near_z = [flip(my_z, i, n_z) for i in range(n_z)]
    near_e = [flip(my_e, i, n_ep) for i in range(n_ep)]
    far_first = near_z[::-1]

    def greet(e, t):
        pl.semaphore_signal(
            barrier,
            inc=1,
            device_id={"ep": e, "tp": t},
            device_id_type=pl.DeviceIdType.MESH,
        )

    def greet_core(i, carry):
        to = lax.rem(my_chip + i, n_chip)
        greet(to // n_z, 2 * lax.rem(to, n_z) + core)
        return carry

    lax.fori_loop(1, n_chip, greet_core, 0)
    for k in range(n_z):
        greet(my_e, 2 * k + 1 - core)

    def remote(src, dst, send_sem, recv_sem, e, t):
        return pltpu.make_async_remote_copy(
            src_ref=src,
            dst_ref=dst,
            send_sem=send_sem,
            recv_sem=recv_sem,
            device_id={"ep": e, "tp": t},
            device_id_type=pl.DeviceIdType.MESH,
        )

    length_load.wait()
    position = jnp.zeros((seqs, 1), F32)
    for s in range(seqs):
        position = jnp.where(iota((seqs, 1), 0) == s, lengths[s].astype(F32), position)
    index = iota((1, rope_width), 1)
    index = jnp.where(index >= half, index - half, index).astype(F32)
    frequency = jnp.power(jnp.full((1, rope_width), ROPE_BASE, F32), -2.0 * index / rope_width)
    angles = position * frequency
    cosine = jnp.cos(angles)
    sine = jnp.sin(angles)
    source = iota((rope_width, rope_width), 0)
    target = iota((rope_width, rope_width), 1)
    turn = (
        jnp.where(source + half == target, 1.0, 0.0) - jnp.where(source == target + half, 1.0, 0.0)
    ).astype(BF16)


    def scores(s):
        query_r = query_rope_v[s]
        turned = (
            query_r.astype(F32) * cosine[s : s + 1] + dot(query_r, turn) * sine[s : s + 1]
        ).astype(BF16)
        score = (dot(query_v[s], cache_v[s], ((1,), (1,))) + dot(turned, rope_v[s])) * scale
        score = jnp.where(iota((heads, length), 1) < lengths[s], score, -jnp.inf)
        return score, turned

    for i in (5, 6):
        loads[i].wait()
    ropes[0].wait()
    caches[0].wait()
    waiting = scores(0)

    for i in (0, 1, 2, 3, 4):
        loads[i].wait()
    resid = residual_v[...].astype(F32)
    gain = norm_gain_v[...].astype(F32).reshape(1, width)
    normed_all = (resid * inverse_rms(resid) * gain).astype(BF16)
    own = jnp.where(
        iota((seqs, rows), 1) == my_t * seqs + iota((seqs, rows), 0), 1.0, 0.0
    ).astype(BF16)
    normed = dot(own, normed_all).astype(BF16)
    latent_raw = dot(normed, latent_weight_v[...])
    new_latent = (
        latent_raw * inverse_rms(latent_raw) * latent_gain_v[...].astype(F32).reshape(1, latent)
    ).astype(BF16)
    weight_r = rope_weight_v[...]
    swapped = jnp.concatenate([-weight_r[half:], weight_r[:half]], axis=0)
    new_rope = (
        dot(normed, weight_r, ((1,), (1,))) * cosine + dot(normed, swapped, ((1,), (1,))) * sine
    ).astype(BF16)
    latent_out[...] = new_latent
    rope_out[...] = new_rope
    new_latent_f = new_latent.astype(F32)
    new_rope_f = new_rope.astype(F32)

    def mix(s, score, turned):
        fresh = (
            jnp.sum(query_v[s].astype(F32) * new_latent_f[s : s + 1], axis=1, keepdims=True)
            + jnp.sum(turned.astype(F32) * new_rope_f[s : s + 1], axis=1, keepdims=True)
        ) * scale
        top = jnp.maximum(jnp.max(score, axis=1, keepdims=True), fresh)
        powers = jnp.exp(score - top)
        fresh_power = jnp.exp(fresh - top)
        inverse = 1.0 / (jnp.sum(powers, axis=1, keepdims=True) + fresh_power)
        fresh_weight = fresh_power.astype(BF16).astype(F32)
        mixed = dot(powers.astype(BF16), cache_v[s]) + fresh_weight * new_latent_f[s : s + 1]
        return (mixed * inverse).astype(BF16)

    mixed_latents = []
    for s in range(1, seqs):
        ropes[s].wait()
        caches[s].wait()
    for kind in expert_loads:
        for load in kind:
            load.start()
    loads[8].wait()
    for s in range(1, seqs):
        found = scores(s)
        mixed_latents.append(mix(s - 1, *waiting))
        waiting = found
    mixed_latents.append(mix(seqs - 1, *waiting))
    lhs = jnp.concatenate(mixed_latents, axis=0)

    for t in range(n_tp):
        found = dot(lhs, value_v[:, t * head_cols : (t + 1) * head_cols])
        head = iota((heads, head_cols), 0)
        column = iota((heads, head_cols), 1) + t * head_cols
        mine = (column >= head * value_dim) & (column < (head + 1) * value_dim)
        block = jnp.zeros((pad, head_cols), F32)
        for s in range(seqs):
            line = jnp.sum(
                jnp.where(mine, found[s * heads : (s + 1) * heads], 0.0), axis=0, keepdims=True
            )
            block = jnp.where(iota((pad, head_cols), 0) == s, line, block)
        head_send[t] = block.astype(BF16)
    pl.semaphore_wait(barrier, n_chip - 1 + n_z)
    for i in reversed(range(1, n_tp)):
        t = flip(my_t, i, n_tp)
        remote(
            head_send.at[t], head_recv.at[my_t], head_sems.at[0, t], head_sems.at[1, my_t], my_e, t
        ).start()
    loads[7].wait()
    id0 = ids_v[0:1, :]
    id1 = ids_v[1:2, :]
    low = iota((n_ep, rows), 0) * local_experts
    high = low + local_experts
    hits = jnp.where(
        ((id0 >= low) & (id0 < high)) | ((id1 >= low) & (id1 < high)), 1.0, 0.0
    ).astype(F32)
    before = jnp.where(iota((rows, rows), 0) < iota((rows, rows), 1), 1.0, 0.0).astype(BF16)
    rank = dot(hits.astype(BF16), before)
    slot_of = jnp.where(hits > 0.5, rank, -1.0)
    slot_row = iota((slots, rows), 0).astype(F32)
    select = jnp.concatenate(
        [jnp.where(slot_row == slot_of[d : d + 1, :], 1.0, 0.0).astype(F32) for d in range(n_ep)],
        axis=0,
    )
    tag0 = jnp.sum(select * (id0.astype(F32) + 1.0), axis=1, keepdims=True)
    tag1 = jnp.sum(select * (id1.astype(F32) + 1.0), axis=1, keepdims=True)
    lane = iota((n_ep * slots, 128), 1)
    tags = jnp.where(lane == 0, tag0, jnp.where(lane == 1, tag1, 0.0))
    for d in range(n_ep):
        meta_send[d] = tags[d * slots : (d + 1) * slots]
    meta_recv[my_e] = meta_send[my_e]
    select_b = select.astype(BF16)

    for i in range(1, n_ep):
        e = lax.rem(my_e + i, n_ep)
        remote(
            meta_send.at[e], meta_recv.at[my_e], meta_sems.at[0, e], meta_sems.at[1, my_e], e, my_t
        ).start()
    head_recv[my_t] = head_send[my_t]
    loads[9].wait()
    line = iota((rows, n_tp * pad), 0)
    spot = iota((rows, n_tp * pad), 1)
    inner = spot & (pad - 1)
    outer = lax.shift_right_logical(spot, pad.bit_length() - 1)
    gather = jnp.where((inner < seqs) & (line == outer * seqs + inner), 1.0, 0.0).astype(BF16)
    for i in range(1, n_tp):
        t = lax.rem(my_t + i, n_tp)
        remote(
            head_send.at[t], head_recv.at[t], head_sems.at[0, t], head_sems.at[1, t], my_e, t
        ).wait()
    by_heads = dot(
        gather, head_recv[...].astype(F32).reshape(n_tp * pad, head_cols).astype(BF16)
    ).astype(BF16)

    def half(send, recv, sems, k):
        return remote(send.at[k], recv.at[k], sems.at[0, k], sems.at[1, k], my_e, sibling)

    def columns(t):
        return pl.ds(pl.multiple_of(t * col, col), col)

    for k in far_first:
        half_send[k] = dot(by_heads, out_v[:, columns(2 * k + 1 - core)]).astype(BF16)
        half(half_send, half_recv, half_sems, k).start()
    parts = [dot(by_heads, out_v[:, columns(2 * k + core)]) for k in far_first]
    for i, k in enumerate(far_first):
        half(half_send, half_recv, half_sems, k).wait()
        attended = parts[i] + half_recv[k].astype(F32)
        if i < n_z - 1:
            sum_send[k] = attended.astype(BF16)
            remote(
                sum_send.at[k],
                sum_recv.at[my_z],
                sum_sems.at[0, k],
                sum_sems.at[1, my_z],
                my_e,
                2 * k + core,
            ).start()
    my_cols = columns(my_t)
    for k in reversed(far_first[:-1]):
        remote(
            sum_send.at[k],
            sum_recv.at[k],
            sum_sems.at[0, k],
            sum_sems.at[1, k],
            my_e,
            2 * k + core,
        ).wait()
        attended = attended + sum_recv[k].astype(F32)
    after = (residual_v[:, my_cols].astype(F32) + attended).astype(BF16)

    chosen = dot(select_b, after).astype(BF16)
    for d in range(n_ep):
        disp_send[d] = chosen[d * slots : (d + 1) * slots]
    disp_recv[my_e, my_t] = disp_send[my_e]

    for i in reversed(range(n_z)):
        for d in reversed(range(n_ep)):
            if i + d > 0:
                e, k = near_e[d], near_z[i]
                remote(
                    disp_send.at[e],
                    disp_recv.at[my_e, my_t],
                    disp_sems.at[0, e, k],
                    disp_sems.at[1, my_e, my_z],
                    e,
                    2 * k + core,
                ).start()
    remote(
        disp_send.at[my_e],
        disp_recv.at[my_e, my_t],
        pass_sems.at[0, my_e, my_z],
        pass_sems.at[1, my_e, my_z],
        my_e,
        sibling,
    ).start()
    for load in loads[10:13]:
        load.wait()

    def pass_rows(e, k):
        return remote(
            disp_recv.at[e, 2 * k + core],
            disp_recv.at[e, 2 * k + core],
            pass_sems.at[0, e, k],
            pass_sems.at[1, e, k],
            my_e,
            sibling,
        )

    def await_rows(i):
        for d in range(n_ep):
            if i + d > 0:
                e, k = near_e[d], near_z[i]
                remote(
                    disp_send.at[e],
                    disp_recv.at[e, 2 * k + core],
                    disp_sems.at[0, e, k],
                    disp_sems.at[1, e, k],
                    e,
                    2 * k + core,
                ).wait()
                pass_rows(e, k).start()

    for i in range(1, n_ep):
        e = near_e[i]
        remote(
            meta_send.at[e], meta_recv.at[e], meta_sems.at[0, e], meta_sems.at[1, e], e, my_t
        ).wait()
    for kind in expert_loads:
        for load in kind:
            load.wait()
    gain_row[...] = mixer_gain_v[...].astype(F32).reshape(1, width)
    total = n_ep * slots
    squares = jnp.zeros((total, 1), F32)
    group_logits = jnp.zeros((total, groups), F32)
    expert_logits = jnp.zeros((total, experts), F32)
    gates = [jnp.zeros((total, gate_v.shape[2]), F32) for _ in range(local_experts)]
    ups = [jnp.zeros((total, gate_v.shape[2]), F32) for _ in range(local_experts)]
    await_rows(0)
    for i in range(n_z):
        if i + 1 < n_z:
            await_rows(i + 1)
        k = near_z[i]
        for d in range(n_ep):
            pass_rows(near_e[d], k).wait()
        span = pl.ds(pl.multiple_of(2 * k * col, 2 * col), 2 * col)
        taken = jnp.concatenate(
            [disp_recv[:, 2 * k + h].reshape(total, col) for h in range(2)], axis=1
        ).astype(F32)
        squares = squares + jnp.sum(taken * taken, axis=1, keepdims=True)
        mixer = gain_row[:, span]
        scaled = (taken * mixer).astype(BF16)
        for l in range(local_experts):
            gates[l] = gates[l] + dot(scaled, gate_v[l, span, :])
            ups[l] = ups[l] + dot(scaled, up_v[l, span, :])
        group_logits = group_logits + dot(scaled, group_router_v[:, span], ((1,), (1,)))
        expert_logits = expert_logits + dot(scaled, expert_router_v[:, span], ((1,), (1,)))
    factor = lax.rsqrt(squares / width + NORM_EPSILON)
    group_logits = group_logits * factor
    expert_logits = expert_logits * factor
    meta = meta_recv[...].reshape(total, 128)
    name0 = meta[:, 0:1] - 1.0
    name1 = meta[:, 1:2] - 1.0
    group_low = (iota((total, groups), 1) * per_group).astype(F32)
    in_group = (name0 >= group_low) & (name0 < group_low + per_group)
    group_top = jnp.sum(jnp.where(in_group, group_logits, 0.0), axis=1, keepdims=True)
    share = 1.0 / jnp.sum(jnp.exp(group_logits - group_top), axis=1, keepdims=True)
    number = iota((total, experts), 1).astype(F32)
    pick0 = jnp.sum(jnp.where(number == name0, expert_logits, 0.0), axis=1, keepdims=True)
    pick1 = jnp.sum(jnp.where(number == name1, expert_logits, 0.0), axis=1, keepdims=True)
    route0 = share / (1.0 + jnp.exp(pick1 - pick0))
    route1 = share / (1.0 + jnp.exp(pick0 - pick1))

    acts = []
    routes = []
    for l in range(local_experts):
        name = (my_e * local_experts + l).astype(F32)
        routes.append(
            jnp.where(name0 == name, route0, 0.0) + jnp.where(name1 == name, route1, 0.0)
        )
        gate = gates[l] * factor
        acts.append((gate / (1.0 + jnp.exp(-gate)) * (ups[l] * factor)).astype(BF16))
    def expert_part(t):
        part = routes[0] * dot(acts[0], down_v[0, :, columns(t)])
        for l in range(1, local_experts):
            part = part + routes[l] * dot(acts[l], down_v[l, :, columns(t)])
        return part

    for k in far_first:
        pair_send[k] = expert_part(2 * k + 1 - core).astype(BF16)
        half(pair_send, pair_recv, pair_sems, k).start()
    for i, k in enumerate(far_first):
        t = 2 * k + core
        part = expert_part(t)
        half(pair_send, pair_recv, pair_sems, k).wait()
        part = (part + pair_recv[k].astype(F32)).astype(BF16)
        for e in range(n_ep):
            ret_send[e, k] = part[e * slots : (e + 1) * slots]
        for d in reversed(range(1 if i == n_z - 1 else 0, n_ep)):
            e = near_e[d]
            remote(
                ret_send.at[e, k],
                ret_recv.at[my_e, my_z],
                ret_sems.at[0, e, k],
                ret_sems.at[1, my_e, my_z],
                e,
                t,
            ).start()
    ret_recv[my_e, my_z] = ret_send[my_e, my_z]

    for i in range(n_z):
        for d in range(n_ep):
            if i + d > 0:
                e, k = near_e[d], near_z[i]
                remote(
                    ret_send.at[e, k],
                    ret_recv.at[e, k],
                    ret_sems.at[0, e, k],
                    ret_sems.at[1, e, k],
                    e,
                    2 * k + core,
                ).wait()
    gathered = ret_recv[:, 0].astype(F32)
    for t in range(1, n_z):
        gathered = gathered + ret_recv[:, t].astype(F32)
    gathered = gathered.reshape(total, col)
    coarse = gathered.astype(BF16)
    fine = (gathered - coarse.astype(F32)).astype(BF16)
    moe = dot(select_b, coarse, ((0,), (0,))) + dot(select_b, fine, ((0,), (0,)))
    share_send[...] = (after.astype(F32) + moe).astype(BF16)
    own_store = pltpu.make_async_copy(share_send, mixed_out.at[:, my_cols], store_sem)
    for i in reversed(range(1, n_tp)):
        t = flip(my_t, i, n_tp)
        remote(
            share_send,
            mixed_out.at[:, my_cols],
            share_sems.at[0, t],
            share_sems.at[1, my_t],
            my_e,
            t,
        ).start()
    own_store.start()
    for i in range(1, n_tp):
        t = flip(my_t, i, n_tp)
        remote(
            share_send,
            mixed_out.at[:, columns(t)],
            share_sems.at[0, t],
            share_sems.at[1, t],
            my_e,
            t,
        ).wait()
    own_store.wait()


def place(arrays):
    count = len(arrays)

    def kernel(*refs):
        copies = [
            pltpu.make_async_copy(refs[i], refs[count + i], refs[-1].at[i]) for i in range(count)
        ]
        for copy in copies:
            copy.start()
        for copy in copies:
            copy.wait()

    arrays = [pltpu.with_memory_space_constraint(a, pltpu.VMEM) for a in arrays]
    return pl.pallas_call(
        kernel,
        out_shape=tuple(jax.ShapeDtypeStruct(a.shape, a.dtype) for a in arrays),
        in_specs=[pl.BlockSpec(memory_space=pltpu.VMEM)] * count,
        out_specs=(pl.BlockSpec(memory_space=pl.ANY),) * count,
        scratch_shapes=[pltpu.SemaphoreType.DMA((count,))],
        name="place",
    )(*arrays)


def on_device(n_ep, n_tp, *args):
    (
        residual,
        cache_latent,
        cache_rope,
        lengths,
        query_latent,
        query_rope,
        norm_gain,
        latent_weight,
        latent_gain,
        rope_weight,
        value_weight,
        out_weight,
        mixer_gain,
        group_router,
        expert_router,
        expert_ids,
        gate_weight,
        up_weight,
        down_weight,
    ) = args
    rows, width = residual.shape
    seqs, heads, latent = query_latent.shape
    rope_width = query_rope.shape[2]
    local_experts = gate_weight.shape[0]
    experts = expert_router.shape[1]
    per_group = experts // group_router.shape[1]
    capacity = 2 * rows * TOPK // experts
    slots = capacity if per_group == TOPK == local_experts else min(local_experts * capacity, rows)
    slots = -(-slots // 16) * 16
    col = width // n_tp
    n_z = n_tp // 2
    head_cols = out_weight.shape[0]
    pad = 8
    while pad < seqs:
        pad *= 2
    value_dim = value_weight.shape[1] // heads
    scale = float((value_dim + rope_width) ** (-0.5))
    group_router = group_router.T
    expert_router = expert_router.T
    expert_ids = expert_ids.T
    hbm = pl.BlockSpec(memory_space=pl.ANY)

    def held(array):
        return pltpu.VMEM(array.shape, array.dtype)

    dma = pltpu.SemaphoreType.DMA
    outs = pl.pallas_call(
        functools.partial(layer, (n_ep, n_tp, slots, scale)),
        out_shape=(
            pltpu.VMEM((rows, width), BF16),
            pltpu.VMEM((seqs, latent), BF16),
            pltpu.VMEM((seqs, rope_width), BF16),
        ),
        in_specs=[hbm] * 19,
        out_specs=(pl.BlockSpec(memory_space=pltpu.VMEM),) * 3,
        scratch_shapes=[
            pltpu.SMEM(lengths.shape, lengths.dtype),
            held(residual),
            held(cache_latent),
            held(cache_rope),
            held(query_latent),
            held(query_rope),
            held(norm_gain),
            held(latent_weight),
            held(latent_gain),
            held(rope_weight),
            held(value_weight),
            held(out_weight),
            held(mixer_gain),
            held(group_router),
            held(expert_router),
            held(expert_ids),
            held(gate_weight),
            held(up_weight),
            held(down_weight),
            pltpu.VMEM((n_tp, pad, head_cols), BF16),
            pltpu.VMEM((n_tp, pad, head_cols), BF16),
            pltpu.VMEM((n_ep, slots, 128), F32),
            pltpu.VMEM((n_ep, slots, 128), F32),
            pltpu.VMEM((n_z, rows, col), BF16),
            pltpu.VMEM((n_z, rows, col), BF16),
            pltpu.VMEM((n_z, rows, col), BF16),
            pltpu.VMEM((n_z, rows, col), BF16),
            pltpu.VMEM((n_ep, slots, col), BF16),
            pltpu.VMEM((n_ep, n_tp, slots, col), BF16),
            pltpu.VMEM((n_z, n_ep * slots, col), BF16),
            pltpu.VMEM((n_z, n_ep * slots, col), BF16),
            pltpu.VMEM((n_ep, n_z, slots, col), BF16),
            pltpu.VMEM((n_ep, n_z, slots, col), BF16),
            pltpu.VMEM((rows, col), BF16),
            pltpu.VMEM((1, width), F32),
            dma,
            dma((13,)),
            dma((seqs,)),
            dma((seqs,)),
            dma((3, local_experts)),
            dma((2, n_tp)),
            dma((2, n_ep)),
            dma((2, n_z)),
            dma((2, n_z)),
            dma((2, n_ep, n_z)),
            dma((2, n_ep, n_z)),
            dma((2, n_z)),
            dma((2, n_ep, n_z)),
            dma((2, n_tp)),
            dma,
        ],
        compiler_params=pltpu.CompilerParams(collective_id=0, has_side_effects=True),
        name="layer",
    )(
        residual,
        cache_latent,
        cache_rope,
        lengths,
        query_latent,
        query_rope,
        norm_gain,
        latent_weight,
        latent_gain,
        rope_weight,
        value_weight,
        out_weight,
        mixer_gain,
        group_router,
        expert_router,
        expert_ids,
        gate_weight,
        up_weight,
        down_weight,
    )
    return place(outs)


def solution(mesh):
    in_specs = (
        P("ep", None),
        P(("ep", "tp"), None, None),
        P(("ep", "tp"), None, None),
        P(("ep", "tp")),
        P(("ep", "tp"), None, None),
        P(("ep", "tp"), None, None),
        P(),
        P(),
        P(),
        P(),
        P(),
        P("tp", None),
        P(),
        P(),
        P(),
        P("ep", None),
        P("ep", None, "tp"),
        P("ep", None, "tp"),
        P("ep", "tp", None),
    )
    out_specs = (P("ep", None), P(("ep", "tp"), None), P(("ep", "tp"), None))
    return jax.shard_map(
        functools.partial(on_device, mesh.shape["ep"], mesh.shape["tp"]),
        mesh=mesh,
        in_specs=in_specs,
        out_specs=out_specs,
        check_vma=False,
    )
```
